32 devices in a mesh: sp: 8 (over z, x), tp: 4 (over y, core).
Axes of the slice: x: 2, y: 2, z: 4, core: 2. Of those that a mesh axis runs over, the one named last changes fastest.
Arguments:
- tokens: bfloat16 [3072, 2048], P('sp'), may hold values from -6 to 6
- doc_ids: int32 [3072], P('sp'), may hold values from 0 to 2, never falling along the last dimension, each value on 1 to 2048 neighbouring positions
- pre_gain: float32 [2, 2048], replicated, may hold values from 0.1 to 1.9
- value_proj: bfloat16 [2, 2048, 1024], P(None, 'sp', 'tp'), may hold values from -0.1875 to 0.1875
- gate_proj: bfloat16 [2, 2048, 1024], P(None, 'sp', 'tp'), may hold values from -0.1875 to 0.1875
- out_proj: bfloat16 [2, 1024, 2048], P(None, 'tp', 'sp'), may hold values from -0.1875 to 0.1875
- conv_taps: float32 [2, 31, 1024], P(None, None, 'tp'), may hold values from -2.2 to 2.2
- norm_gain: float32 [2, 1024], P(None, 'tp'), may hold values from 0.1 to 1.9
- norm_shift: float32 [2, 1024], P(None, 'tp'), may hold values from -3 to 3
Outputs:
- hidden: bfloat16 [3072, 2048], P('sp')
The draws below stay inside these ranges and needn't reach their ends.
Inputs may be any that keep to these rules, and one draw needn't show every extreme that they name: `doc_ids`: document numbers never fall along the sequence; each document has 1 to 2048 positions.
All inputs are finite; a program needn't handle non-finite values.
Results may differ from the reference program's by a relative error of at most 0.017.
Values may be sent and summed in bfloat16 or wider, within the bound.
A program may use at most 64 MiB of HBM per device.

```python
import math
import jax
import jax.numpy as jnp
import numpy as np
from jax import lax

D = 2048
C = 1024
KW = 31
LAYERS = 2
TOKENS = 3072
DOCS = 3
DOC_MOST = 2048
N_TP = 4


def draw_conv_taps(key, part):
    scale_key = jax.random.fold_in(key, 11)
    tap_key = jax.random.fold_in(key, 12)
    group_scale = jnp.exp(jax.random.uniform(scale_key, (8,), jnp.float32, jnp.log(0.25), jnp.log(4.0)))
    channel_scale = jnp.repeat(group_scale, C // 8)
    raw = jnp.clip(jax.random.normal(tap_key, (LAYERS, KW, C), jnp.float32), -3.0, 3.0)
    return raw * channel_scale[None, None, :] / jnp.sqrt(jnp.float32(KW))


def spiked(drawn, stream_key, source, target, parts, factor):
    owner, partner = [(jnp.arange(drawn.shape[dim]) // (drawn.shape[dim] // parts)).reshape([-1 if axis == dim else 1 for axis in range(drawn.ndim)]) for dim in (source, target)]
    chosen = jax.random.permutation(stream_key, parts)[partner]
    strong = (owner == chosen) | (owner == (partner + parts // 2) % parts)
    return jnp.where(strong, factor * drawn, drawn)


def levels(rng, dims, shards, smallest, high):
    factor_of, own = 1.0, jax.random.fold_in(rng, 6)
    for dim, parts in shards:
        heights = jnp.exp(jax.random.uniform(jax.random.fold_in(own, dim), (parts,), jnp.float32, smallest / len(shards), high / len(shards)))
        factor_of = factor_of * jnp.repeat(heights, dims[dim] // parts).reshape([-1 if axis == dim else 1 for axis in range(len(dims))])
    return factor_of


def length_profile(count, total, most, lean):
    portions = [(1 << 20) // math.isqrt(rank ** lean) + 1 for rank in range(2, count + 1)]
    rest, holding = total - most - (count - 1), [1] * (count - 1)
    while rest > 0:
        movable = [i for i in range(count - 1) if holding[i] < most]
        whole, remaining = sum([portions[i] for i in movable]), rest
        for i in movable:
            extra = min(most - holding[i], max(1, remaining * portions[i] // whole), rest)
            holding[i] = holding[i] + extra
            rest = rest - extra
    return np.array([most] + holding)


def ragged_sizes(own_key, number_of, total, limit, slope):
    if number_of == 2:
        one = jax.random.randint(own_key, (), max(1, total - limit), min(limit, total - 1) + 1)
        return jnp.stack([one, total - one])
    sizes = jnp.asarray(length_profile(number_of, total, limit, slope), jnp.int32)
    couples = (number_of - 1) // 2
    giver, receiver = sizes[1:1 + 2 * couples:2], sizes[2:2 + 2 * couples:2]
    margin = jnp.minimum(giver - 1, limit - receiver)
    passed = jax.random.randint(jax.random.fold_in(own_key, 1), (couples,), 0, 1 << 20) % (margin + 1)
    sizes = sizes.at[1:1 + 2 * couples:2].set(giver - passed).at[2:2 + 2 * couples:2].set(receiver + passed)
    return sizes[jax.random.permutation(jax.random.fold_in(own_key, 2), number_of)]


def scatter_about(rng, extent, scale, most, cuts=(), held_as=jnp.bfloat16):
    array = scale * jax.random.normal(rng, extent, jnp.float32)
    if cuts:
        array = array * levels(rng, extent, cuts, -0.22, 0.18)
    return jnp.clip(array, -most, most).astype(held_as)


def gaussian_with(rng, dims, scale, limit, cuts, heavy, dtype=jnp.bfloat16):
    array = scale * jax.random.normal(rng, dims, jnp.float32)
    if cuts:
        array = array * levels(rng, dims, cuts, -0.22, 0.18)
    return jnp.clip(spiked(array, jax.random.fold_in(rng, 3), *heavy), -limit, limit).astype(dtype)


def setup_inputs(seed: int = 0) -> dict:
    seeds = jax.random.split(jax.random.key(seed), 10)
    tokens = scatter_about(seeds[0], (TOKENS, D), 1.0, 6.0, ((0, 8),))
    doc_ids = jnp.searchsorted(jnp.cumsum(ragged_sizes(seeds[1], DOCS, TOKENS, DOC_MOST, 0)), jnp.arange(TOKENS), side="right").astype(jnp.int32)
    pre_gain = jnp.clip(1.0 + 0.18 * jax.random.normal(seeds[2], (LAYERS, D), jnp.float32), 0.1, 1.9)
    value_proj = gaussian_with(seeds[3], (LAYERS, D, C), D ** -0.5, 0.1875, ((1, 8), (2, 4)), (1, 2, 8, 2.0))
    gate_proj = gaussian_with(seeds[4], (LAYERS, D, C), D ** -0.5, 0.1875, ((1, 8), (2, 4)), (1, 2, 8, 2.0))
    out_proj = scatter_about(seeds[5], (LAYERS, C, D), C ** -0.5, 0.1875, ((1, 4), (2, 8)))
    conv_taps = draw_conv_taps(jax.random.fold_in(seeds[9], 71), 0)
    norm_gain = jnp.clip(1.0 + 0.18 * jax.random.normal(seeds[7], (LAYERS, C), jnp.float32), 0.1, 1.9)
    norm_shift = scatter_about(seeds[8], (LAYERS, C), 0.5, 3.0, ((1, 4),), jnp.float32)
    return dict(tokens=tokens, doc_ids=doc_ids, pre_gain=pre_gain, value_proj=value_proj, gate_proj=gate_proj, out_proj=out_proj, conv_taps=conv_taps, norm_gain=norm_gain, norm_shift=norm_shift)


epsilon = 1e-06

def reference(tokens, doc_ids, pre_gain, value_proj, gate_proj, out_proj, conv_taps, norm_gain, norm_shift):
    hidden = tokens
    padded_docs = jnp.concatenate([jnp.full((KW - 1,), -1, jnp.int32), doc_ids.astype(jnp.int32)])
    block_width = C // N_TP
    for layer_index in range(LAYERS):
        wide_state = hidden.astype(jnp.float32)
        scale = lax.rsqrt(lax.optimization_barrier(jnp.mean(wide_state * wide_state, axis=-1, keepdims=True)) + epsilon)
        normed = (wide_state * scale * pre_gain[layer_index]).astype(jnp.bfloat16)
        value_half = jnp.dot(normed, value_proj[layer_index], preferred_element_type=jnp.float32).astype(jnp.bfloat16)
        gate_half = jnp.dot(normed, gate_proj[layer_index], preferred_element_type=jnp.float32).astype(jnp.bfloat16)
        gated_rows = (value_half.astype(jnp.float32) * jax.nn.sigmoid(gate_half.astype(jnp.float32))).astype(jnp.bfloat16)
        padded = jnp.concatenate([jnp.zeros((KW - 1, C), jnp.bfloat16), gated_rows]).astype(jnp.float32)
        conv_out = jnp.zeros((TOKENS, C), jnp.float32)
        for offset in range(KW):
            first_row = KW - 1 - offset
            same_doc = (padded_docs[first_row:first_row + TOKENS] == doc_ids)[:, None]
            term = conv_taps[layer_index, offset][None, :] * padded[first_row:first_row + TOKENS]
            conv_out = conv_out + jnp.where(same_doc, term, jnp.float32(0.0))
        row_mean = lax.optimization_barrier(jnp.mean(conv_out, axis=-1, keepdims=True))
        row_var = lax.optimization_barrier(jnp.mean(jnp.square(conv_out - row_mean), axis=-1, keepdims=True))
        normalized = norm_gain[layer_index] * (conv_out - row_mean) * lax.rsqrt(row_var + epsilon) + norm_shift[layer_index]
        activated = jax.nn.silu(normalized).astype(jnp.bfloat16)
        total = jnp.zeros((TOKENS, D), jnp.float32)
        for block_index in range(N_TP):
            lower = block_index * block_width
            share = jnp.dot(activated[:, lower:lower + block_width], out_proj[layer_index, lower:lower + block_width], preferred_element_type=jnp.float32)
            total = total + share.astype(jnp.bfloat16).astype(jnp.float32)
        branch = total.astype(jnp.bfloat16)
        hidden = (hidden.astype(jnp.float32) + branch.astype(jnp.float32)).astype(jnp.bfloat16)
    return hidden
```

```python
import functools
import jax
import jax.numpy as jnp
from jax import lax
from jax.experimental import pallas as pl
from jax.experimental.pallas import tpu as pltpu
from jax.sharding import PartitionSpec as P

epsilon = 1e-06
MESH = pl.DeviceIdType.MESH
HALO = 32
CONV_ROWS = 64


def fused_kernel(
    n, m, reach, layers,
    tok_ref, doc_ref, gain_ref, v_ref, g_ref, o_ref, tap_ref, ng_ref, ns_ref,
    out_ref,
    w, oring, ofull, normed, acc, padded, pdoc, run, ghalo, halo_in, doc_in, doc_tail,
    stat, stat_out, stat_in, conv, act_all, hid,
    rsend, rrecv, osend, orecv, hsend, hrecv, ssend, srecv, asend, arecv, xsend, xrecv,
):
    me = lax.axis_index("sp")
    t = lax.axis_index("tp")
    q, c = t // 2, t % 2
    pairs = m // 2
    half_n = n // 2
    rows, width = tok_ref.shape
    depth, block = v_ref.shape[1], v_ref.shape[2]
    owidth = o_ref.shape[2]
    hb, ho = block // 2, owidth // 2
    half_width = width // 2
    channels = block * m

    def index_of(position):
        position = (position + 2 * n) % n
        return jnp.where(position < half_n, 2 * position, 2 * (n - 1 - position) + 1)

    my_pos = jnp.where(me % 2 == 0, me // 2, n - 1 - me // 2)
    right, left = index_of(my_pos + 1), index_of(my_pos - 1)
    following = (me + 1) % n

    barrier = pltpu.get_barrier_semaphore()
    for other in (right, left):
        pl.semaphore_signal(barrier, inc=1, device_id={"sp": other}, device_id_type=MESH)
    for k in range(1, m):
        pl.semaphore_signal(barrier, inc=1, device_id={"tp": (t + k) % m}, device_id_type=MESH)
    pl.semaphore_wait(barrier, 1 + m)

    def to_sp(src, dst, send, recv, target):
        return pltpu.make_async_remote_copy(
            src_ref=src, dst_ref=dst, send_sem=send, recv_sem=recv,
            device_id={"sp": target}, device_id_type=MESH)

    def to_tp(src, dst, send, recv, target):
        return pltpu.make_async_remote_copy(
            src_ref=src, dst_ref=dst, send_sem=send, recv_sem=recv,
            device_id={"tp": target}, device_id_type=MESH)

    def owner_at(way, distance):
        return index_of(my_pos - distance if way == 0 else my_pos + distance)

    def held(layer, kind, owner, piece):
        if kind < 2:
            return w.at[layer, kind, pl.ds(pl.multiple_of(owner * depth, depth), depth), pl.ds(piece * hb, hb)]
        return oring.at[layer, :, pl.ds(pl.multiple_of(owner * owidth + piece * ho, ho), ho)]

    def own_piece(layer, kind, piece):
        if kind < 2:
            return (v_ref, g_ref)[piece].at[layer, :, pl.ds(kind * hb, hb)]
        return o_ref.at[layer, :, pl.ds(piece * ho, ho)]

    def ring_copy(layer, kind, way, step, piece, src, dst):
        return to_sp(src, dst, rsend.at[layer, kind, way, step, piece], rrecv.at[layer, kind, way, step, piece],
                     right if way == 0 else left)

    def travels(way, step, piece):
        return step < half_n - 1 or piece == way

    def spread_copy(layer, way, step, piece, pair):
        owner = owner_at(way, step)
        part = owner // half_n
        local = owner - part * half_n
        src = own_piece(layer, 2, piece) if step == 0 else held(layer, 2, owner, piece)
        dst = ofull.at[layer, pl.ds(pl.multiple_of(t * block, block), block),
                       pl.ds(pl.multiple_of(local * owidth + piece * ho, ho), ho)]
        copy = to_tp(src, dst, osend.at[layer, way, step, piece, pair],
                     orecv.at[layer, t, local * 2 + piece], 2 * ((q + pair) % pairs) + part)
        return copy, part

    def spread(layer, way, step, piece, act):
        for pair in range(pairs - 1, -1, -1):
            copy, part = spread_copy(layer, way, step, piece, pair)
            if pair == 0:
                pl.when(part != c)(lambda copy=copy: getattr(copy, act)())
            else:
                getattr(copy, act)()

    def advance_one(layer, kind, step):
        for piece in range(2):
            for way in range(2):
                if step > 0:
                    if not travels(way, step - 1, piece):
                        continue
                    piece_ref = held(layer, kind, owner_at(way, step), piece)
                    ring_copy(layer, kind, way, step - 1, piece, piece_ref, piece_ref).wait_recv()
                if step < half_n and travels(way, step, piece):
                    dst = held(layer, kind, owner_at(way, step), piece)
                    src = own_piece(layer, kind, piece) if step == 0 else dst
                    ring_copy(layer, kind, way, step, piece, src, dst).start()
            if kind == 2:
                for way in range(2):
                    if step == 0 and way == 1 or step > 0 and not travels(way, step - 1, piece):
                        continue
                    spread(layer, way, step, piece, "start")

    entries = []
    for layer in range(layers):
        for step in range(half_n + 1):
            entries.append((11 * layer + 3.3 * step, layer, 0, step))
            entries.append((11 * layer + (2 if layer else 1) + 3.3 * step, layer, 1, step))
            entries.append((11 * layer + 5 + 3.2 * step, layer, 2, step))
    pending = [entry[1:] for entry in sorted(entries)]

    def tend(count):
        for _ in range(count):
            if pending:
                advance_one(*pending.pop(0))

    def advance(*target):
        while target in pending:
            advance_one(*pending.pop(0))

    def keep_own(layer):
        row = pl.ds(pl.multiple_of(me * depth, depth), depth)
        for kind in range(2):
            w[layer, kind, row, pl.ds(0, hb)] = v_ref[layer, :, kind * hb:(kind + 1) * hb]
            w[layer, kind, row, pl.ds(hb, hb)] = g_ref[layer, :, kind * hb:(kind + 1) * hb]
        oring[layer, :, pl.ds(pl.multiple_of(me * owidth, owidth), owidth)] = o_ref[layer]

    tend(2)

    def doc_block(i):
        row = doc_ref[pl.ds(i, 1), :].astype(jnp.float32)
        return jnp.transpose(jnp.broadcast_to(row, (128, 128)))

    doc_tail[...] = doc_block(rows // 128 - 1)[128 - HALO:]
    doc_copy = to_sp(doc_tail, doc_in, hsend.at[2 * layers], hrecv.at[2 * layers], following)

    for i in range(rows // 128):
        pdoc[pl.ds(HALO + i * 128, 128), :] = doc_block(i)
    pdoc[pl.ds(0, HALO), :] = jnp.full((HALO, 128), -1.0, jnp.float32)

    def norm_rows(layer, source):
        @pl.loop(0, rows // 32)
        def _(i):
            span = pl.ds(pl.multiple_of(i * 32, 32), 32)
            wide = source[span, :].astype(jnp.float32)
            scale = lax.rsqrt(jnp.mean(wide * wide, axis=-1, keepdims=True) + epsilon)
            normed[span, :] = (wide * scale * gain_ref[pl.ds(layer, 1), :]).astype(jnp.bfloat16)

    norm_rows(0, tok_ref)
    for layer in range(layers):
        keep_own(layer)

    @pl.when(me == 0)
    def _():
        halo_in[...] = jnp.zeros(halo_in.shape, halo_in.dtype)


    def count_runs():
        @pl.when(me > 0)
        def _():
            doc_copy.wait_recv()
            pdoc[pl.ds(0, HALO), :] = doc_in[...]

        @pl.loop(0, rows // CONV_ROWS)
        def _(i):
            base = pl.multiple_of(i * CONV_ROWS, CONV_ROWS)
            mine = pdoc[pl.ds(base + HALO, CONV_ROWS), :]
            count = jnp.zeros((CONV_ROWS, 128), jnp.int32)
            for j in range(1, reach + 1):
                count = count + (pdoc[pl.ds(base + (HALO - j), CONV_ROWS), :] == mine).astype(jnp.int32)
            run[pl.ds(base, CONV_ROWS), :] = count

    lane = lax.broadcasted_iota(jnp.int32, (CONV_ROWS, 128), 1)

    def layer_step(layer, source, target):
        last = layer + 1 == layers

        def halo_copy(kind):
            return to_sp(ghalo.at[layer, kind], halo_in.at[layer, kind],
                         hsend.at[2 * layer + kind], hrecv.at[2 * layer + kind], following)

        def store_padded(kind, row, values):
            padded[kind, pl.ds(row, 32), :] = values.astype(jnp.float32)

        def gate_half(kind):
            acc[...] = jnp.dot(normed[...], w[layer, kind], preferred_element_type=jnp.float32)

            def gate_rows(i):
                span = pl.ds(pl.multiple_of(i * 32, 32), 32)
                value = acc[span, pl.ds(0, hb)].astype(jnp.bfloat16).astype(jnp.float32)
                gate = acc[span, pl.ds(hb, hb)].astype(jnp.bfloat16).astype(jnp.float32)
                gated = (value * jax.nn.sigmoid(gate)).astype(jnp.bfloat16)
                store_padded(kind, pl.multiple_of(i * 32 + HALO, 32), gated)
                return gated

            ghalo[layer, kind] = gate_rows(rows // 32 - 1)
            pl.when(me < n - 1)(lambda: halo_copy(kind).start())

            @pl.loop(0, rows // 32 - 1)
            def _(i):
                gate_rows(i)

        def conv_half(kind):
            pl.when(me > 0)(lambda: halo_copy(kind).wait_recv())
            store_padded(kind, 0, halo_in[layer, kind])
            cols = pl.ds(kind * hb, hb)

            @pl.loop(0, rows // CONV_ROWS)
            def _(i):
                base = pl.multiple_of(i * CONV_ROWS, CONV_ROWS)
                count = run[pl.ds(base, CONV_ROWS), :]
                total = tap_ref[0, pl.ds(layer, 1), cols] * padded[kind, pl.ds(base + HALO, CONV_ROWS), :]
                for j in range(1, reach + 1):
                    term = tap_ref[j, pl.ds(layer, 1), cols] * padded[kind, pl.ds(base + (HALO - j), CONV_ROWS), :]
                    total = total + jnp.where(count >= j, term, jnp.float32(0.0))
                conv[pl.ds(base, CONV_ROWS), cols] = total
                sums = jnp.where(
                    lane == 0, jnp.sum(total, axis=1, keepdims=True),
                    jnp.where(lane == 1, jnp.sum(total * total, axis=1, keepdims=True), jnp.float32(0.0)))
                if kind:
                    sums = sums + stat[pl.ds(base, CONV_ROWS), :]
                stat[pl.ds(base, CONV_ROWS), :] = sums

        advance(layer, 0, half_n)
        if layer == 0:
            pl.when(me < n - 1)(doc_copy.start)
        gate_half(0)
        if last:
            tend(1)
            conv_half(0)
        advance(layer, 1, half_n)
        gate_half(1)
        if layer == 0:
            count_runs()
        if last:
            advance(layer, 2, half_n)
        else:
            tend(1)
            conv_half(0)
            tend(1)
        conv_half(1)

        stat_out[layer] = jnp.transpose(stat[...])[:8]
        stat_copies = [
            to_tp(stat_out.at[layer], stat_in.at[layer, t], ssend.at[layer, k], srecv.at[layer, t], (t + k) % m)
            for k in range(1, m)]
        for copy in stat_copies:
            copy.start()
        if not last:
            tend(1)
        summed = stat_out[layer]
        for k in range(1, m):
            peer = (t + k) % m
            to_tp(stat_in.at[layer, peer], stat_in.at[layer, peer], ssend.at[layer, k],
                  srecv.at[layer, peer], peer).wait_recv()
            summed = summed + stat_in[layer, peer]
        stat[...] = jnp.transpose(
            jnp.concatenate([summed, jnp.zeros((120, rows), jnp.float32)], axis=0))

        mine = pl.ds(pl.multiple_of(t * block, block), block)

        @pl.loop(0, rows // CONV_ROWS)
        def _(i):
            span = pl.ds(pl.multiple_of(i * CONV_ROWS, CONV_ROWS), CONV_ROWS)
            both = stat[span, :]
            row_mean = both[:, 0:1] / channels
            row_var = both[:, 1:2] / channels - row_mean * row_mean
            normalized = (ng_ref[pl.ds(layer, 1), :] * (conv[span, :] - row_mean)
                          * lax.rsqrt(row_var + epsilon) + ns_ref[pl.ds(layer, 1), :])
            act_all[layer, span, mine] = jax.nn.silu(normalized).astype(jnp.bfloat16)

        def act_cols(who):
            return act_all.at[layer, :, pl.ds(pl.multiple_of(who * block, block), block)]

        partner = 2 * q + 1 - c
        copies = []
        for k in range(pairs - 1, -1, -1):
            target_t = 2 * ((q + k) % pairs) + c if k else partner
            copies.append(to_tp(act_cols(t), act_cols(t), asend.at[layer, k], arecv.at[layer, t], target_t))
            copies[-1].start()
        if not last:
            tend(2)
        for k in range(1, pairs):
            sender = 2 * ((q + k) % pairs) + c
            to_tp(act_cols(sender), act_cols(sender), asend.at[layer, k], arecv.at[layer, sender], sender).wait_recv()
            copies.append(to_tp(act_cols(sender), act_cols(sender), asend.at[layer, pairs + k],
                                arecv.at[layer, sender], partner))
            copies[-1].start()
        if not last:
            advance(layer, 2, half_n)
            tend(1)
        ofull[layer, pl.ds(pl.multiple_of(t * block, block), block), :] = oring[
            layer, :, pl.ds(pl.multiple_of(c * half_width, half_width), half_width)]
        for k in range(1, m):
            peer = (t + k) % m

            @pl.loop(0, n)
            def _(piece, peer=peer):
                dst = ofull.at[layer, pl.ds(pl.multiple_of(peer * block, block), block),
                               pl.ds(pl.multiple_of(piece * ho, ho), ho)]
                to_tp(dst, dst, osend.at[layer, 0, 0, 0, 0], orecv.at[layer, peer, piece], peer).wait_recv()

        for k in range(pairs):
            sender = 2 * ((q + k) % pairs) + 1 - c
            to_tp(act_cols(sender), act_cols(sender), asend.at[layer, k], arecv.at[layer, sender], partner).wait_recv()
        half = pl.ds(pl.multiple_of(c * half_width, half_width), half_width)
        branch = jnp.dot(act_all[layer], ofull[layer], preferred_element_type=jnp.float32).astype(jnp.bfloat16)
        target[:, half] = (source[:, half].astype(jnp.float32) + branch.astype(jnp.float32)).astype(jnp.bfloat16)
        swap = to_tp(target.at[:, half], target.at[:, half], xsend.at[layer], xrecv.at[layer], partner)
        swap.start()
        if not last:
            tend(1)
        swap.wait_recv()
        if not last:
            norm_rows(layer + 1, target)
            tend(1)
        for copy in copies + stat_copies:
            copy.wait_send()
        for kind in range(2):
            pl.when(me < n - 1)(lambda kind=kind: halo_copy(kind).wait_send())
        swap.wait_send()

    for layer in range(layers):
        layer_step(layer, tok_ref if layer == 0 else hid.at[layer - 1], hid.at[layer])
    out_ref[...] = hid[layers - 1]

    pl.when(me < n - 1)(doc_copy.wait_send)

    for layer in range(layers):
        for way in range(2):
            for piece in range(2):
                for kind in range(3):
                    @pl.loop(0, half_n if piece == way else half_n - 1)
                    def _(step, layer=layer, way=way, piece=piece, kind=kind):
                        ref = held(layer, kind, me, piece)
                        ring_copy(layer, kind, way, step, piece, ref, ref).wait_send()

                @pl.loop(1 if way else 0, half_n + 1 if piece == way else half_n)
                def _(step, layer=layer, way=way, piece=piece):
                    for pair in range(pairs):
                        part = owner_at(way, step) // half_n
                        ref = held(layer, 2, me, piece)
                        copy = to_tp(ref, ref, osend.at[layer, way, step, piece, pair],
                                     orecv.at[layer, t, 0], 2 * ((q + pair) % pairs) + part)
                        if pair == 0:
                            pl.when(part != c)(copy.wait_send)
                        else:
                            copy.wait_send()


def fused_on_device(n, m, tokens, doc_ids, pre_gain, value_proj, gate_proj, out_proj, conv_taps, norm_gain, norm_shift):
    rows, width = tokens.shape
    layers, depth, block = value_proj.shape
    owidth = out_proj.shape[2]
    reach = conv_taps.shape[1] - 1
    channels = block * m
    docs = doc_ids.reshape(rows // 128, 128)
    bf16, f32, i32 = jnp.bfloat16, jnp.float32, jnp.int32
    dma = pltpu.SemaphoreType.DMA
    vmem = pl.BlockSpec(memory_space=pltpu.VMEM)
    return pl.pallas_call(
        functools.partial(fused_kernel, n, m, reach, layers),
        out_shape=jax.ShapeDtypeStruct((rows, width), bf16),
        in_specs=[vmem] * 9,
        out_specs=vmem,
        scratch_shapes=[
            pltpu.VMEM((layers, 2, n * depth, block), bf16),
            pltpu.VMEM((layers, block, n * owidth), bf16),
            pltpu.VMEM((layers, channels, width // 2), bf16),
            pltpu.VMEM((rows, width), bf16),
            pltpu.VMEM((rows, block), f32),
            pltpu.VMEM((2, rows + HALO, block // 2), f32),
            pltpu.VMEM((rows + HALO, 128), f32),
            pltpu.VMEM((rows, 128), i32),
            pltpu.VMEM((layers, 2, HALO, block // 2), bf16),
            pltpu.VMEM((layers, 2, HALO, block // 2), bf16),
            pltpu.VMEM((HALO, 128), f32),
            pltpu.VMEM((HALO, 128), f32),
            pltpu.VMEM((rows, 128), f32),
            pltpu.VMEM((layers, 8, rows), f32),
            pltpu.VMEM((layers, m, 8, rows), f32),
            pltpu.VMEM((rows, block), f32),
            pltpu.VMEM((layers, rows, channels), bf16),
            pltpu.VMEM((layers, rows, width), bf16),
            dma((layers, 3, 2, n // 2, 2)), dma((layers, 3, 2, n // 2, 2)),
            dma((layers, 2, n // 2 + 1, 2, m // 2)), dma((layers, m, n)),
            dma((2 * layers + 1,)), dma((2 * layers + 1,)),
            dma((layers, m)), dma((layers, m)),
            dma((layers, m)), dma((layers, m)),
            dma((layers,)), dma((layers,)),
        ],
        compiler_params=pltpu.CompilerParams(
            collective_id=0, has_side_effects=True, vmem_limit_bytes=60 * 1024 * 1024),
    )(tokens, docs, pre_gain, value_proj, gate_proj, out_proj, jnp.transpose(conv_taps, (1, 0, 2)), norm_gain, norm_shift)


def passed_along(value, axis, steps):
    count = lax.axis_size(axis)
    first, last = (max(0, -steps), min(count, count - steps))
    return lax.ppermute(value, axis, [(source, source + steps) for source in range(first, last)])


def on_device(
    tokens, doc_ids, pre_gain, value_proj, gate_proj, out_proj, conv_taps, norm_gain, norm_shift
):
    layer_count = value_proj.shape[0]
    tap_count = conv_taps.shape[1]
    reach_rows = tap_count - 1
    row_count = tokens.shape[0]
    block_width = conv_taps.shape[2]
    channels = block_width * lax.axis_size("tp")
    hidden = tokens
    full_value, full_gate, full_out = (
        lax.all_gather(value_proj, "sp", axis=1, tiled=True),
        lax.all_gather(gate_proj, "sp", axis=1, tiled=True),
        lax.all_gather(out_proj, "sp", axis=2, tiled=True),
    )
    for layer_index in range(layer_count):
        wide_state = hidden.astype(jnp.float32)
        scale = lax.rsqrt(jnp.mean(wide_state * wide_state, axis=-1, keepdims=True) + epsilon)
        normed = (wide_state * scale * pre_gain[layer_index]).astype(jnp.bfloat16)
        value_acc = jnp.dot(normed, full_value[layer_index], preferred_element_type=jnp.float32)
        gate_acc = jnp.dot(normed, full_gate[layer_index], preferred_element_type=jnp.float32)
        value_half = value_acc.astype(jnp.bfloat16)
        gate_half = gate_acc.astype(jnp.bfloat16)
        gated_rows = (
            value_half.astype(jnp.float32) * jax.nn.sigmoid(gate_half.astype(jnp.float32))
        ).astype(jnp.bfloat16)
        prev_rows, prev_docs = passed_along(
            (gated_rows[row_count - reach_rows :], doc_ids[row_count - reach_rows :]), "sp", 1
        )
        padded = jnp.concatenate([prev_rows, gated_rows]).astype(jnp.float32)
        padded_docs = jnp.concatenate([prev_docs, doc_ids])
        conv_out = jnp.zeros((row_count, block_width), jnp.float32)
        for offset in range(tap_count):
            first_row = reach_rows - offset
            same_doc = (padded_docs[first_row : first_row + row_count] == doc_ids)[:, None]
            term = (
                conv_taps[layer_index, offset][None, :] * padded[first_row : first_row + row_count]
            )
            conv_out = conv_out + jnp.where(same_doc, term, jnp.float32(0.0))
        row_sums, square_sums = lax.psum(
            (jnp.sum(conv_out, axis=1), jnp.sum(conv_out * conv_out, axis=1)), "tp"
        )
        row_mean = (row_sums / channels)[:, None]
        row_var = (square_sums / channels)[:, None] - row_mean * row_mean
        normalized = (
            norm_gain[layer_index] * (conv_out - row_mean) * lax.rsqrt(row_var + epsilon)
            + norm_shift[layer_index]
        )
        activated = jax.nn.silu(normalized).astype(jnp.bfloat16)
        partial_value = jnp.dot(
            activated, full_out[layer_index], preferred_element_type=jnp.float32
        )
        summed = lax.psum(partial_value.astype(jnp.bfloat16), "tp")
        hidden = (hidden.astype(jnp.float32) + summed.astype(jnp.float32)).astype(jnp.bfloat16)
    return hidden


def suits_kernel(n, m, tokens, value_proj, out_proj, conv_taps):
    rows, width = tokens.shape
    depth, block = value_proj.shape[1:]
    return (
        n % 2 == 0 and 4 <= n <= 16 and m % 2 == 0 and m >= 4 and rows % 128 == 0 and width % 256 == 0
        and depth % 32 == 0 and block == 256 and out_proj.shape[2] % 256 == 0
        and conv_taps.shape[1] - 1 <= HALO
    )


def solution(mesh):
    n, m = mesh.shape["sp"], mesh.shape["tp"]

    def body(tokens, doc_ids, pre_gain, value_proj, gate_proj, out_proj, conv_taps, norm_gain, norm_shift):
        chosen = on_device
        if suits_kernel(n, m, tokens, value_proj, out_proj, conv_taps):
            chosen = functools.partial(fused_on_device, n, m)
        return chosen(tokens, doc_ids, pre_gain, value_proj, gate_proj, out_proj, conv_taps, norm_gain, norm_shift)

    return jax.shard_map(
        body,
        mesh=mesh,
        in_specs=(
            P("sp", None),
            P("sp"),
            P(),
            P(None, "sp", "tp"),
            P(None, "sp", "tp"),
            P(None, "tp", "sp"),
            P(None, None, "tp"),
            P(None, "tp"),
            P(None, "tp"),
        ),
        out_specs=P("sp", None),
        check_vma=False,
    )
```

```python
import functools
import jax
import jax.numpy as jnp
from jax import lax
from jax.experimental import pallas as pl
from jax.experimental.pallas import tpu as pltpu
from jax.sharding import PartitionSpec as P

epsilon = 1e-06
MESH = pl.DeviceIdType.MESH
HALO = 32
CONV_ROWS = 64


def fused_kernel(
    n, m, reach, layers,
    tok_ref, doc_ref, gain_ref, v_ref, g_ref, o_ref, tap_ref, ng_ref, ns_ref,
    out_ref,
    w, oall, normed, acc, padded, pdoc, run, ghalo, halo_in, doc_in, doc_tail,
    stat, stats, ng_all, ns_all, conv, act, psend, precv, hid,
    rsend, rrecv, osend, orecv, hsend, hrecv, ssend, srecv, csend, crecv, xsend, xrecv, gsend, grecv, wsem,
):
    me = lax.axis_index("sp")
    t = lax.axis_index("tp")
    q, c = t // 2, t % 2
    pairs = m // 2
    half_n = n // 2
    rows, width = tok_ref.shape
    depth, block = v_ref.shape[1], v_ref.shape[2]
    owidth = o_ref.shape[2]
    hb, ho = block // 2, owidth // 2
    channels = block * m

    def index_of(position):
        position = (position + 2 * n) % n
        return jnp.where(position < half_n, 2 * position, 2 * (n - 1 - position) + 1)

    my_pos = jnp.where(me % 2 == 0, me // 2, n - 1 - me // 2)
    right, left = index_of(my_pos + 1), index_of(my_pos - 1)
    following = (me + 1) % n

    barrier = pltpu.get_barrier_semaphore()
    for other in (right, left):
        pl.semaphore_signal(barrier, inc=1, device_id={"sp": other}, device_id_type=MESH)
    for k in range(1, m):
        pl.semaphore_signal(barrier, inc=1, device_id={"tp": (t + k) % m}, device_id_type=MESH)
    pl.semaphore_wait(barrier, 1 + m)

    def to_sp(src, dst, send, recv, target):
        return pltpu.make_async_remote_copy(
            src_ref=src, dst_ref=dst, send_sem=send, recv_sem=recv,
            device_id={"sp": target}, device_id_type=MESH)

    def to_tp(src, dst, send, recv, target):
        return pltpu.make_async_remote_copy(
            src_ref=src, dst_ref=dst, send_sem=send, recv_sem=recv,
            device_id={"tp": target}, device_id_type=MESH)

    def owner_at(way, distance):
        return index_of(my_pos - distance if way == 0 else my_pos + distance)

    def held(layer, kind, owner, piece):
        if kind < 2:
            return w.at[layer, kind, pl.ds(pl.multiple_of(owner * depth, depth), depth), pl.ds(piece * hb, hb)]
        return oall.at[layer, pl.ds(pl.multiple_of(q * block, block), block),
                       pl.ds(pl.multiple_of(owner * owidth + piece * ho, ho), ho)]

    def own_piece(layer, kind, piece):
        if kind < 2:
            return (v_ref, g_ref)[piece].at[layer, :, pl.ds(kind * hb, hb)]
        return o_ref.at[layer, :, pl.ds(piece * ho, ho)]

    def ring_copy(layer, kind, way, step, piece, src, dst):
        return to_sp(src, dst, rsend.at[layer, kind, way, step, piece], rrecv.at[layer, kind, way, step, piece],
                     right if way == 0 else left)

    def travels(way, step, piece):
        return step < half_n - 1 or piece == way

    def spread(layer, way, step, piece, act):
        owner = owner_at(way, step)
        part = held(layer, 2, owner, piece)
        src = own_piece(layer, 2, piece) if step == 0 else part
        for k in range(1, pairs):
            copy = to_tp(src, part, osend.at[layer, way, step, piece, k - 1],
                         orecv.at[layer, q, owner * 2 + piece], 2 * ((q + k) % pairs) + c)
            getattr(copy, act)()

    def advance_one(layer, kind, step):
        for turn in range(2):
            for way in range(2):
                piece = turn ^ way
                arrived = step == 0 or travels(way, step - 1, piece)
                if step > 0 and arrived:
                    piece_ref = held(layer, kind, owner_at(way, step), piece)
                    ring_copy(layer, kind, way, step - 1, piece, piece_ref, piece_ref).wait_recv()
                if step < half_n and travels(way, step, piece):
                    dst = held(layer, kind, owner_at(way, step), piece)
                    src = own_piece(layer, kind, piece) if step == 0 else dst
                    ring_copy(layer, kind, way, step, piece, src, dst).start()
                if kind == 2 and arrived and (step > 0 or way == 0):
                    spread(layer, way, step, piece, "start")

    entries = []
    for layer in range(layers):
        for step in range(half_n + 1):
            entries.append((11 * layer + 3.3 * step, layer, 0, step))
            entries.append((11 * layer + (2 if layer else 1) + 3.3 * step, layer, 1, step))
            entries.append((11 * layer + (2.5 if layer else 5) + 3.2 * step, layer, 2, step))
    pending = [entry[1:] for entry in sorted(entries)]

    def tend(count):
        for _ in range(count):
            if pending:
                advance_one(*pending.pop(0))

    def advance(*target):
        while target in pending:
            advance_one(*pending.pop(0))

    def keep_own(layer):
        row = pl.ds(pl.multiple_of(me * depth, depth), depth)
        for kind in range(2):
            w[layer, kind, row, pl.ds(0, hb)] = v_ref[layer, :, kind * hb:(kind + 1) * hb]
            w[layer, kind, row, pl.ds(hb, hb)] = g_ref[layer, :, kind * hb:(kind + 1) * hb]
        oall[layer, pl.ds(pl.multiple_of(q * block, block), block),
             pl.ds(pl.multiple_of(me * owidth, owidth), owidth)] = o_ref[layer]

    tend(2)
    gain_copies = []
    for k in range(1, pairs):
        for index, (src, dst) in enumerate(((ng_ref, ng_all), (ns_ref, ns_all))):
            copy = to_tp(src, dst.at[q], gsend.at[k, index], grecv.at[q, index], 2 * ((q + k) % pairs) + c)
            copy.start()
            gain_copies.append(copy)
    ng_all[q] = ng_ref[...]
    ns_all[q] = ns_ref[...]

    def doc_block(i):
        row = doc_ref[pl.ds(i, 1), :].astype(jnp.float32)
        return jnp.transpose(jnp.broadcast_to(row, (128, 128)))

    doc_tail[...] = doc_block(rows // 128 - 1)[128 - HALO:]
    doc_copy = to_sp(doc_tail, doc_in, hsend.at[2 * layers], hrecv.at[2 * layers], following)

    for i in range(rows // 128):
        pdoc[pl.ds(HALO + i * 128, 128), :] = doc_block(i)
    pdoc[pl.ds(0, HALO), :] = jnp.full((HALO, 128), -1.0, jnp.float32)

    def norm_rows(layer, source):
        @pl.loop(0, rows // 32)
        def _(i):
            span = pl.ds(pl.multiple_of(i * 32, 32), 32)
            wide = source[span, :].astype(jnp.float32)
            scale = lax.rsqrt(jnp.mean(wide * wide, axis=-1, keepdims=True) + epsilon)
            normed[span, :] = (wide * scale * gain_ref[pl.ds(layer, 1), :]).astype(jnp.bfloat16)

    norm_rows(0, tok_ref)
    for layer in range(layers):
        keep_own(layer)

    @pl.when(me == 0)
    def _():
        halo_in[...] = jnp.zeros(halo_in.shape, halo_in.dtype)


    def count_runs():
        for k in range(1, pairs):
            for index, dst in enumerate((ng_all, ns_all)):
                peer = (q + k) % pairs
                to_tp(dst.at[peer], dst.at[peer], gsend.at[k, index], grecv.at[peer, index], t).wait_recv()

        @pl.when(me > 0)
        def _():
            doc_copy.wait_recv()
            pdoc[pl.ds(0, HALO), :] = doc_in[...]

        @pl.loop(0, rows // CONV_ROWS)
        def _(i):
            base = pl.multiple_of(i * CONV_ROWS, CONV_ROWS)
            mine = pdoc[pl.ds(base + HALO, CONV_ROWS), :]
            count = jnp.zeros((CONV_ROWS, 128), jnp.int32)
            for j in range(1, reach + 1):
                count = count + (pdoc[pl.ds(base + (HALO - j), CONV_ROWS), :] == mine).astype(jnp.int32)
            run[pl.ds(base, CONV_ROWS), :] = count

    lane = lax.broadcasted_iota(jnp.int32, (CONV_ROWS, 128), 1)
    chunks = rows // 128
    order = list(range(1, chunks)) + [0]
    partner = 2 * q + 1 - c

    def layer_step(layer, source, target):
        last = layer + 1 == layers
        marks = [1, 1, 1, 1, 1, 1, 1, 1, 1]

        def pause():
            if not last and marks:
                tend(marks.pop(0))

        def halo_copy(kind):
            return to_sp(ghalo.at[layer, kind], halo_in.at[layer, kind],
                         hsend.at[2 * layer + kind], hrecv.at[2 * layer + kind], following)

        def store_padded(kind, row, values):
            padded[kind, pl.ds(row, 32), :] = values.astype(jnp.float32)

        def gate_half(kind):
            acc[...] = jnp.dot(normed[...], w[layer, kind], preferred_element_type=jnp.float32)

            def gate_rows(i):
                span = pl.ds(pl.multiple_of(i * 32, 32), 32)
                value = acc[span, pl.ds(0, hb)].astype(jnp.bfloat16).astype(jnp.float32)
                gate = acc[span, pl.ds(hb, hb)].astype(jnp.bfloat16).astype(jnp.float32)
                gated = (value * jax.nn.sigmoid(gate)).astype(jnp.bfloat16)
                store_padded(kind, pl.multiple_of(i * 32 + HALO, 32), gated)
                return gated

            ghalo[layer, kind] = gate_rows(rows // 32 - 1)
            pl.when(me < n - 1)(lambda: halo_copy(kind).start())

            @pl.loop(0, rows // 32 - 1)
            def _(i):
                gate_rows(i)

        def take_halo(kind):
            pl.when(me > 0)(lambda: halo_copy(kind).wait_recv())
            store_padded(kind, 0, halo_in[layer, kind])

        def conv_rows(kind, first, end):
            cols = pl.ds(kind * hb, hb)

            @pl.loop(first, end)
            def _(i):
                base = pl.multiple_of(i * CONV_ROWS, CONV_ROWS)
                span = pl.ds(base, CONV_ROWS)
                count = run[span, :]
                total = tap_ref[0, pl.ds(layer, 1), cols] * padded[kind, pl.ds(base + HALO, CONV_ROWS), :]
                for j in range(1, reach + 1):
                    term = tap_ref[j, pl.ds(layer, 1), cols] * padded[kind, pl.ds(base + (HALO - j), CONV_ROWS), :]
                    total = total + jnp.where(count >= j, term, jnp.float32(0.0))
                conv[layer, q, span, cols] = total.astype(jnp.bfloat16)
                sums = jnp.where(
                    lane == 0, jnp.sum(total, axis=1, keepdims=True),
                    jnp.where(lane == 1, jnp.sum(total * total, axis=1, keepdims=True), jnp.float32(0.0)))
                if kind:
                    sums = sums + stat[span, :]
                stat[span, :] = sums

        def conv_copies(kind, chunk, p, act):
            span = pl.ds(chunk * 128, 128) if kind else pl.ds(0, rows)
            slot = chunk + 1 if kind else 0
            for k in range(1, pairs):
                peer = (q + k) % pairs
                part = conv.at[layer, p if p is not None else peer, span, pl.ds(kind * hb, hb)]
                copy = to_tp(part, part, csend.at[layer, k, slot],
                             crecv.at[layer, p if p is not None else peer, slot], 2 * peer + c)
                getattr(copy, act)()

        def stat_copy(chunk, k, who):
            part = stats.at[layer, who, chunk]
            return to_tp(part, part, ssend.at[layer, k, chunk], srecv.at[layer, who, chunk], (t + k) % m)

        def swap_copy(chunk):
            span = pl.ds(chunk * 128, 128)
            return to_tp(psend.at[layer, span], precv.at[layer, span], xsend.at[layer, chunk],
                         xrecv.at[layer, chunk], partner)

        def first_half():
            conv_rows(0, 1, rows // CONV_ROWS)
            take_halo(0)
            conv_rows(0, 0, 1)
            conv_copies(0, 0, q, "start")

        advance(layer, 0, half_n)
        if layer == 0:
            pl.when(me < n - 1)(doc_copy.start)
        gate_half(0)
        if last:
            tend(1)
            first_half()
        advance(layer, 1, half_n)
        gate_half(1)
        if last:
            advance(layer, 2, half_n)
        else:
            if layer == 0:
                count_runs()
            pause()
            first_half()
        for chunk in order:
            if chunk == 0:
                pause()
                take_halo(1)
            conv_rows(1, 2 * chunk, 2 * chunk + 2)
            stats[layer, t, chunk] = jnp.transpose(stat[pl.ds(chunk * 128, 128), :])[:8]
            for k in range(1, m):
                stat_copy(chunk, k, t).start()
            conv_copies(1, chunk, q, "start")

        pause()
        pause()
        gains = [ng_all[p, pl.ds(layer, 1), :] for p in range(pairs)]
        shifts = [ns_all[p, pl.ds(layer, 1), :] for p in range(pairs)]
        for chunk in order:
            for k in range(1, m):
                stat_copy(chunk, k, (t + k) % m).wait_recv()
            summed = stats[layer, 0, chunk]
            for who in range(1, m):
                summed = summed + stats[layer, who, chunk]
            both = jnp.transpose(jnp.concatenate([summed, jnp.zeros((120, 128), jnp.float32)], axis=0))
            row_mean = both[:, 0:1] / channels
            row_var = both[:, 1:2] / channels - row_mean * row_mean
            row_scale = lax.rsqrt(row_var + epsilon)
            if chunk == order[0]:
                conv_copies(0, 0, None, "wait_recv")
            conv_copies(1, chunk, None, "wait_recv")
            span = pl.ds(chunk * 128, 128)
            for p in range(pairs):
                normalized = gains[p] * (conv[layer, p, span, :].astype(jnp.float32) - row_mean) * row_scale + shifts[p]
                act[span, pl.ds(p * block, block)] = jax.nn.silu(normalized).astype(jnp.bfloat16)
            if chunk == order[0]:
                if not last:
                    pause()
                    advance(layer, 2, half_n)
                for k in range(1, pairs):
                    peer = (q + k) % pairs

                    @pl.loop(0, 2 * n)
                    def _(piece, peer=peer):
                        part = oall.at[layer, pl.ds(pl.multiple_of(peer * block, block), block),
                                       pl.ds(pl.multiple_of(piece * ho, ho), ho)]
                        to_tp(part, part, osend.at[layer, 0, 0, 0, 0], orecv.at[layer, peer, piece], t).wait_recv()
            psend[layer, span, :] = jnp.dot(
                act[span, :], oall[layer], preferred_element_type=jnp.float32).astype(jnp.bfloat16)
            swap_copy(chunk).start()
            pause()

        for chunk in order:
            swap_copy(chunk).wait_recv()

            @pl.loop(0, 128 // 32)
            def _(i, chunk=chunk):
                span = pl.ds(pl.multiple_of(chunk * 128 + i * 32, 32), 32)
                branch = (psend[layer, span, :].astype(jnp.float32)
                          + precv[layer, span, :].astype(jnp.float32)).astype(jnp.bfloat16)
                total = (source[span, :].astype(jnp.float32) + branch.astype(jnp.float32)).astype(jnp.bfloat16)
                target[span, :] = total
                if not last:
                    wide = total.astype(jnp.float32)
                    scale = lax.rsqrt(jnp.mean(wide * wide, axis=-1, keepdims=True) + epsilon)
                    normed[span, :] = (wide * scale * gain_ref[pl.ds(layer + 1, 1), :]).astype(jnp.bfloat16)

            if last:
                span = pl.ds(chunk * 128, 128)
                pltpu.make_async_copy(target.at[span], out_ref.at[span], wsem.at[chunk]).start()
            pause()

        for chunk in range(chunks):
            for k in range(1, m):
                stat_copy(chunk, k, t).wait_send()
            conv_copies(1, chunk, q, "wait_send")
            swap_copy(chunk).wait_send()
        conv_copies(0, 0, q, "wait_send")
        for kind in range(2):
            pl.when(me < n - 1)(lambda kind=kind: halo_copy(kind).wait_send())

    for layer in range(layers):
        layer_step(layer, tok_ref if layer == 0 else hid.at[layer - 1], hid.at[layer])
    for copy in gain_copies:
        copy.wait_send()

    pl.when(me < n - 1)(doc_copy.wait_send)

    for layer in range(layers):
        for way in range(2):
            for piece in range(2):
                for kind in range(3):
                    @pl.loop(0, half_n if piece == way else half_n - 1)
                    def _(step, layer=layer, way=way, piece=piece, kind=kind):
                        ref = held(layer, kind, me, piece)
                        ring_copy(layer, kind, way, step, piece, ref, ref).wait_send()

                @pl.loop(1 if way else 0, half_n + 1 if piece == way else half_n)
                def _(step, layer=layer, way=way, piece=piece):
                    for k in range(1, pairs):
                        ref = held(layer, 2, me, piece)
                        to_tp(ref, ref, osend.at[layer, way, step, piece, k - 1],
                              orecv.at[layer, q, 0], 2 * ((q + k) % pairs) + c).wait_send()

    for chunk in range(chunks):
        span = pl.ds(chunk * 128, 128)
        pltpu.make_async_copy(hid.at[layers - 1, span], out_ref.at[span], wsem.at[chunk]).wait()


def fused_on_device(n, m, tokens, doc_ids, pre_gain, value_proj, gate_proj, out_proj, conv_taps, norm_gain, norm_shift):
    rows, width = tokens.shape
    layers, depth, block = value_proj.shape
    owidth = out_proj.shape[2]
    reach = conv_taps.shape[1] - 1
    pairs, chunks = m // 2, rows // 128
    docs = doc_ids.reshape(rows // 128, 128)
    bf16, f32, i32 = jnp.bfloat16, jnp.float32, jnp.int32
    dma = pltpu.SemaphoreType.DMA
    vmem = pl.BlockSpec(memory_space=pltpu.VMEM)
    return pl.pallas_call(
        functools.partial(fused_kernel, n, m, reach, layers),
        out_shape=jax.ShapeDtypeStruct((rows, width), bf16),
        in_specs=[vmem] * 9,
        out_specs=pl.BlockSpec(memory_space=pl.ANY),
        scratch_shapes=[
            pltpu.VMEM((layers, 2, n * depth, block), bf16),
            pltpu.VMEM((layers, pairs * block, n * owidth), bf16),
            pltpu.VMEM((rows, width), bf16),
            pltpu.VMEM((rows, block), f32),
            pltpu.VMEM((2, rows + HALO, block // 2), f32),
            pltpu.VMEM((rows + HALO, 128), f32),
            pltpu.VMEM((rows, 128), i32),
            pltpu.VMEM((layers, 2, HALO, block // 2), bf16),
            pltpu.VMEM((layers, 2, HALO, block // 2), bf16),
            pltpu.VMEM((HALO, 128), f32),
            pltpu.VMEM((HALO, 128), f32),
            pltpu.VMEM((rows, 128), f32),
            pltpu.VMEM((layers, m, chunks, 8, 128), f32),
            pltpu.VMEM((pairs, layers, block), f32),
            pltpu.VMEM((pairs, layers, block), f32),
            pltpu.VMEM((layers, pairs, rows, block), bf16),
            pltpu.VMEM((rows, pairs * block), bf16),
            pltpu.VMEM((layers, rows, width), bf16),
            pltpu.VMEM((layers, rows, width), bf16),
            pltpu.VMEM((layers, rows, width), bf16),
            dma((layers, 3, 2, n // 2, 2)), dma((layers, 3, 2, n // 2, 2)),
            dma((layers, 2, n // 2 + 1, 2, pairs)), dma((layers, pairs, 2 * n)),
            dma((2 * layers + 1,)), dma((2 * layers + 1,)),
            dma((layers, m, chunks)), dma((layers, m, chunks)),
            dma((layers, pairs, chunks + 1)), dma((layers, pairs, chunks + 1)),
            dma((layers, chunks)), dma((layers, chunks)),
            dma((pairs, 2)), dma((pairs, 2)), dma((chunks,)),
        ],
        compiler_params=pltpu.CompilerParams(
            collective_id=0, has_side_effects=True, vmem_limit_bytes=60 * 1024 * 1024),
    )(tokens, docs, pre_gain, value_proj, gate_proj, out_proj, jnp.transpose(conv_taps, (1, 0, 2)), norm_gain, norm_shift)


def passed_along(value, axis, steps):
    count = lax.axis_size(axis)
    first, last = (max(0, -steps), min(count, count - steps))
    return lax.ppermute(value, axis, [(source, source + steps) for source in range(first, last)])


def on_device(
    tokens, doc_ids, pre_gain, value_proj, gate_proj, out_proj, conv_taps, norm_gain, norm_shift
):
    layer_count = value_proj.shape[0]
    tap_count = conv_taps.shape[1]
    reach_rows = tap_count - 1
    row_count = tokens.shape[0]
    block_width = conv_taps.shape[2]
    channels = block_width * lax.axis_size("tp")
    hidden = tokens
    full_value, full_gate, full_out = (
        lax.all_gather(value_proj, "sp", axis=1, tiled=True),
        lax.all_gather(gate_proj, "sp", axis=1, tiled=True),
        lax.all_gather(out_proj, "sp", axis=2, tiled=True),
    )
    for layer_index in range(layer_count):
        wide_state = hidden.astype(jnp.float32)
        scale = lax.rsqrt(jnp.mean(wide_state * wide_state, axis=-1, keepdims=True) + epsilon)
        normed = (wide_state * scale * pre_gain[layer_index]).astype(jnp.bfloat16)
        value_acc = jnp.dot(normed, full_value[layer_index], preferred_element_type=jnp.float32)
        gate_acc = jnp.dot(normed, full_gate[layer_index], preferred_element_type=jnp.float32)
        value_half = value_acc.astype(jnp.bfloat16)
        gate_half = gate_acc.astype(jnp.bfloat16)
        gated_rows = (
            value_half.astype(jnp.float32) * jax.nn.sigmoid(gate_half.astype(jnp.float32))
        ).astype(jnp.bfloat16)
        prev_rows, prev_docs = passed_along(
            (gated_rows[row_count - reach_rows :], doc_ids[row_count - reach_rows :]), "sp", 1
        )
        padded = jnp.concatenate([prev_rows, gated_rows]).astype(jnp.float32)
        padded_docs = jnp.concatenate([prev_docs, doc_ids])
        conv_out = jnp.zeros((row_count, block_width), jnp.float32)
        for offset in range(tap_count):
            first_row = reach_rows - offset
            same_doc = (padded_docs[first_row : first_row + row_count] == doc_ids)[:, None]
            term = (
                conv_taps[layer_index, offset][None, :] * padded[first_row : first_row + row_count]
            )
            conv_out = conv_out + jnp.where(same_doc, term, jnp.float32(0.0))
        row_sums, square_sums = lax.psum(
            (jnp.sum(conv_out, axis=1), jnp.sum(conv_out * conv_out, axis=1)), "tp"
        )
        row_mean = (row_sums / channels)[:, None]
        row_var = (square_sums / channels)[:, None] - row_mean * row_mean
        normalized = (
            norm_gain[layer_index] * (conv_out - row_mean) * lax.rsqrt(row_var + epsilon)
            + norm_shift[layer_index]
        )
        activated = jax.nn.silu(normalized).astype(jnp.bfloat16)
        partial_value = jnp.dot(
            activated, full_out[layer_index], preferred_element_type=jnp.float32
        )
        summed = lax.psum(partial_value.astype(jnp.bfloat16), "tp")
        hidden = (hidden.astype(jnp.float32) + summed.astype(jnp.float32)).astype(jnp.bfloat16)
    return hidden


def suits_kernel(n, m, tokens, value_proj, out_proj, conv_taps):
    rows, width = tokens.shape
    depth, block = value_proj.shape[1:]
    return (
        n % 2 == 0 and 4 <= n <= 16 and m % 2 == 0 and m >= 4 and rows % 128 == 0 and width % 256 == 0
        and depth % 32 == 0 and block == 256 and out_proj.shape[2] % 256 == 0
        and conv_taps.shape[1] - 1 <= HALO
    )


def solution(mesh):
    n, m = mesh.shape["sp"], mesh.shape["tp"]

    def body(tokens, doc_ids, pre_gain, value_proj, gate_proj, out_proj, conv_taps, norm_gain, norm_shift):
        chosen = on_device
        if suits_kernel(n, m, tokens, value_proj, out_proj, conv_taps):
            chosen = functools.partial(fused_on_device, n, m)
        return chosen(tokens, doc_ids, pre_gain, value_proj, gate_proj, out_proj, conv_taps, norm_gain, norm_shift)

    return jax.shard_map(
        body,
        mesh=mesh,
        in_specs=(
            P("sp", None),
            P("sp"),
            P(),
            P(None, "sp", "tp"),
            P(None, "sp", "tp"),
            P(None, "tp", "sp"),
            P(None, None, "tp"),
            P(None, "tp"),
            P(None, "tp"),
        ),
        out_specs=P("sp", None),
        check_vma=False,
    )
```

```python
import functools
import jax
import jax.numpy as jnp
from jax import lax
from jax.experimental import pallas as pl
from jax.experimental.pallas import tpu as pltpu
from jax.sharding import PartitionSpec as P

epsilon = 1e-06
MESH = pl.DeviceIdType.MESH
HALO = 32
CONV_ROWS = 64


def fused_kernel(
    n, m, reach, layers,
    tok_hbm, doc_hbm, gain_hbm, v_hbm, g_hbm, o_hbm, tap_hbm, ng_hbm, ns_hbm,
    out_ref, tok_ref, doc_ref, gain_ref, v_ref, g_ref, o_ref, tap_ref, ng_ref, ns_ref,
    w, oall, normed, acc, padded, pdoc, run, ghalo, halo_in, doc_in, doc_tail,
    stat, stats, ng_all, ns_all, conv, act, psend, precv, hid,
    rsend, rrecv, osend, orecv, hsend, hrecv, ssend, srecv, csend, crecv, xsend, xrecv, gsend, grecv, lsem,
):
    me = lax.axis_index("sp")
    t = lax.axis_index("tp")
    q, c = t // 2, t % 2
    pairs = m // 2
    half_n = n // 2
    rows, width = tok_ref.shape
    depth, block = v_ref.shape[1], v_ref.shape[2]
    owidth = o_ref.shape[2]
    hb, ho = block // 2, owidth // 2
    channels = block * m

    def index_of(position):
        position = (position + 2 * n) % n
        return jnp.where(position < half_n, 2 * position, 2 * (n - 1 - position) + 1)

    my_pos = jnp.where(me % 2 == 0, me // 2, n - 1 - me // 2)
    right, left = index_of(my_pos + 1), index_of(my_pos - 1)
    following = (me + 1) % n

    barrier = pltpu.get_barrier_semaphore()
    for other in (right, left):
        pl.semaphore_signal(barrier, inc=1, device_id={"sp": other}, device_id_type=MESH)
    for k in range(1, m):
        pl.semaphore_signal(barrier, inc=1, device_id={"tp": (t + k) % m}, device_id_type=MESH)
    loads = [pltpu.make_async_copy(src, dst, lsem.at[index]) for index, (src, dst) in enumerate(
        ((v_hbm, v_ref), (g_hbm, g_ref), (o_hbm, o_ref), (ng_hbm, ng_ref), (ns_hbm, ns_ref),
         (tok_hbm, tok_ref), (gain_hbm, gain_ref), (doc_hbm, doc_ref), (tap_hbm, tap_ref)))]
    for load in loads:
        load.start()
    pl.semaphore_wait(barrier, 1 + m)

    def to_sp(src, dst, send, recv, target):
        return pltpu.make_async_remote_copy(
            src_ref=src, dst_ref=dst, send_sem=send, recv_sem=recv,
            device_id={"sp": target}, device_id_type=MESH)

    def to_tp(src, dst, send, recv, target):
        return pltpu.make_async_remote_copy(
            src_ref=src, dst_ref=dst, send_sem=send, recv_sem=recv,
            device_id={"tp": target}, device_id_type=MESH)

    def owner_at(way, distance):
        return index_of(my_pos - distance if way == 0 else my_pos + distance)

    def held(layer, kind, owner, piece):
        if kind < 2:
            return w.at[layer, kind, pl.ds(pl.multiple_of(owner * depth, depth), depth), pl.ds(piece * hb, hb)]
        return oall.at[layer, pl.ds(pl.multiple_of(q * block, block), block),
                       pl.ds(pl.multiple_of(owner * owidth + piece * ho, ho), ho)]

    def own_piece(layer, kind, piece):
        if kind < 2:
            return (v_ref, g_ref)[piece].at[layer, :, pl.ds(kind * hb, hb)]
        return o_ref.at[layer, :, pl.ds(piece * ho, ho)]

    def ring_copy(layer, kind, way, step, piece, src, dst):
        return to_sp(src, dst, rsend.at[layer, kind], rrecv.at[layer, kind, way, step, piece],
                     right if way == 0 else left)

    def travels(way, step, piece):
        return step < half_n - 1 or piece == way

    def spread(layer, way, step, piece):
        owner = owner_at(way, step)
        part = held(layer, 2, owner, piece)
        src = own_piece(layer, 2, piece) if step == 0 else part
        for k in range(1, pairs):
            to_tp(src, part, osend.at[layer, k], orecv.at[layer, q], 2 * ((q + k) % pairs) + c).start()

    def advance_one(layer, kind, step):
        for turn in range(2):
            for way in range(2):
                piece = turn ^ way
                arrived = step == 0 or travels(way, step - 1, piece)
                if step > 0 and arrived:
                    piece_ref = held(layer, kind, owner_at(way, step), piece)
                    ring_copy(layer, kind, way, step - 1, piece, piece_ref, piece_ref).wait_recv()
                if step < half_n and travels(way, step, piece):
                    dst = held(layer, kind, owner_at(way, step), piece)
                    src = own_piece(layer, kind, piece) if step == 0 else dst
                    ring_copy(layer, kind, way, step, piece, src, dst).start()
                if kind == 2 and arrived and step > 0:
                    spread(layer, way, step, piece)

    entries = []
    for layer in range(layers):
        for step in range(half_n + 1):
            for kind, (first, base, pace) in enumerate(
                    ((10.5, 10.5, 3.5), (13.5, 11.9, 3.4), (12.2, 11.5, 3.4)) if layer
                    else ((0, 0, 3), (1, 1, 3), (0.5, 0.5, 3))):
                shift = 11.5 * max(layer - 1, 0)
                entries.append((shift + (base + pace * step if step else first), layer, kind, step))
    pending = [entry[1:] for entry in sorted(entries)]

    def tend(count):
        for _ in range(count):
            if pending:
                advance_one(*pending.pop(0))

    def advance(*target):
        while target in pending:
            advance_one(*pending.pop(0))

    def drain(layer):
        for kind in range(3):
            if kind < 2:
                ref = w.at[layer, kind, pl.ds(0, (n - 1) * depth)]
            else:
                ref = oall.at[layer, pl.ds(pl.multiple_of(q * block, block), block), pl.ds(0, (n - 1) * owidth)]
            to_sp(ref, ref, rsend.at[layer, kind], rrecv.at[layer, kind, 0, 0, 0], right).wait_send()
        for k in range(1, pairs):
            ref = oall.at[layer, pl.ds(pl.multiple_of(q * block, block), block)]
            to_tp(ref, ref, osend.at[layer, k], orecv.at[layer, q], 2 * ((q + k) % pairs) + c).wait_send()

    def keep_own(layer):
        row = pl.ds(pl.multiple_of(me * depth, depth), depth)
        for kind in range(2):
            w[layer, kind, row, pl.ds(0, hb)] = v_ref[layer, :, kind * hb:(kind + 1) * hb]
            w[layer, kind, row, pl.ds(hb, hb)] = g_ref[layer, :, kind * hb:(kind + 1) * hb]
        oall[layer, pl.ds(pl.multiple_of(q * block, block), block),
             pl.ds(pl.multiple_of(me * owidth, owidth), owidth)] = o_ref[layer]

    for load in loads[:5]:
        load.wait()
    tend(3)
    for layer in range(layers):
        for piece in range(2):
            spread(layer, 0, 0, piece)
    gain_copies = []
    for k in range(1, pairs):
        for index, (src, dst) in enumerate(((ng_ref, ng_all), (ns_ref, ns_all))):
            copy = to_tp(src, dst.at[q], gsend.at[k, index], grecv.at[q, index], 2 * ((q + k) % pairs) + c)
            copy.start()
            gain_copies.append(copy)
    ng_all[q] = ng_ref[...]
    ns_all[q] = ns_ref[...]

    for load in loads[5:]:
        load.wait()

    def doc_block(i):
        row = doc_ref[pl.ds(i, 1), :].astype(jnp.float32)
        return jnp.transpose(jnp.broadcast_to(row, (128, 128)))

    doc_tail[...] = doc_block(rows // 128 - 1)[128 - HALO:]
    doc_copy = to_sp(doc_tail, doc_in, hsend.at[2 * layers], hrecv.at[2 * layers], following)

    for i in range(rows // 128):
        pdoc[pl.ds(HALO + i * 128, 128), :] = doc_block(i)
    pdoc[pl.ds(0, HALO), :] = jnp.full((HALO, 128), -1.0, jnp.float32)

    def norm_rows(layer, source):
        @pl.loop(0, rows // 32)
        def _(i):
            span = pl.ds(pl.multiple_of(i * 32, 32), 32)
            wide = source[span, :].astype(jnp.float32)
            scale = lax.rsqrt(jnp.mean(wide * wide, axis=-1, keepdims=True) + epsilon)
            normed[span, :] = (wide * scale * gain_ref[pl.ds(layer, 1), :]).astype(jnp.bfloat16)

    norm_rows(0, tok_ref)
    for layer in range(layers):
        keep_own(layer)

    @pl.when(me == 0)
    def _():
        halo_in[...] = jnp.zeros(halo_in.shape, halo_in.dtype)


    def count_runs():
        for k in range(1, pairs):
            for index, dst in enumerate((ng_all, ns_all)):
                peer = (q + k) % pairs
                to_tp(dst.at[peer], dst.at[peer], gsend.at[k, index], grecv.at[peer, index], t).wait_recv()

        @pl.when(me > 0)
        def _():
            doc_copy.wait_recv()
            pdoc[pl.ds(0, HALO), :] = doc_in[...]

        @pl.loop(0, rows // CONV_ROWS)
        def _(i):
            base = pl.multiple_of(i * CONV_ROWS, CONV_ROWS)
            mine = pdoc[pl.ds(base + HALO, CONV_ROWS), :]
            count = jnp.zeros((CONV_ROWS, 128), jnp.int32)
            for j in range(1, reach + 1):
                count = count + (pdoc[pl.ds(base + (HALO - j), CONV_ROWS), :] == mine).astype(jnp.int32)
            run[pl.ds(base, CONV_ROWS), :] = count

    lane = lax.broadcasted_iota(jnp.int32, (CONV_ROWS, 128), 1)
    chunks = rows // 128
    order = list(range(1, chunks)) + [0]
    partner = 2 * q + 1 - c

    def layer_step(layer, source, target):
        last = layer + 1 == layers
        marks = [1, 1, 1, 1, 1, 1, 1, 1, 1]

        def pause():
            if not last and marks:
                tend(marks.pop(0))

        def halo_copy(kind):
            return to_sp(ghalo.at[layer, kind], halo_in.at[layer, kind],
                         hsend.at[2 * layer + kind], hrecv.at[2 * layer + kind], following)

        def store_padded(kind, row, values):
            padded[kind, pl.ds(row, 32), :] = values.astype(jnp.float32)

        def gate_half(kind):
            acc[...] = jnp.dot(normed[...], w[layer, kind], preferred_element_type=jnp.float32)

            def gate_rows(i):
                span = pl.ds(pl.multiple_of(i * 32, 32), 32)
                value = acc[span, pl.ds(0, hb)].astype(jnp.bfloat16).astype(jnp.float32)
                gate = acc[span, pl.ds(hb, hb)].astype(jnp.bfloat16).astype(jnp.float32)
                gated = (value * jax.nn.sigmoid(gate)).astype(jnp.bfloat16)
                store_padded(kind, pl.multiple_of(i * 32 + HALO, 32), gated)
                return gated

            ghalo[layer, kind] = gate_rows(rows // 32 - 1)
            pl.when(me < n - 1)(lambda: halo_copy(kind).start())

            @pl.loop(0, rows // 32 - 1)
            def _(i):
                gate_rows(i)

        def take_halo(kind):
            pl.when(me > 0)(lambda: halo_copy(kind).wait_recv())
            store_padded(kind, 0, halo_in[layer, kind])

        def conv_rows(kind, first, end):
            cols = pl.ds(kind * hb, hb)

            @pl.loop(first, end)
            def _(i):
                base = pl.multiple_of(i * CONV_ROWS, CONV_ROWS)
                span = pl.ds(base, CONV_ROWS)
                count = run[span, :]
                total = tap_ref[0, pl.ds(layer, 1), cols] * padded[kind, pl.ds(base + HALO, CONV_ROWS), :]
                for j in range(1, reach + 1):
                    term = tap_ref[j, pl.ds(layer, 1), cols] * padded[kind, pl.ds(base + (HALO - j), CONV_ROWS), :]
                    total = total + jnp.where(count >= j, term, jnp.float32(0.0))
                conv[layer, q, span, cols] = total.astype(jnp.bfloat16)
                sums = jnp.where(
                    lane == 0, jnp.sum(total, axis=1, keepdims=True),
                    jnp.where(lane == 1, jnp.sum(total * total, axis=1, keepdims=True), jnp.float32(0.0)))
                if kind:
                    sums = sums + stat[span, :]
                stat[span, :] = sums

        def conv_copies(kind, chunk, p, act):
            span = pl.ds(chunk * 128, 128) if kind else pl.ds(0, rows)
            slot = chunk + 1 if kind else 0
            for k in range(1, pairs):
                peer = (q + k) % pairs
                part = conv.at[layer, p if p is not None else peer, span, pl.ds(kind * hb, hb)]
                copy = to_tp(part, part, csend.at[layer, k, slot],
                             crecv.at[layer, p if p is not None else peer, slot], 2 * peer + c)
                getattr(copy, act)()

        def stat_copy(chunk, k, who):
            part = stats.at[layer, who, chunk]
            return to_tp(part, part, ssend.at[layer, k, chunk], srecv.at[layer, who, chunk], (t + k) % m)

        def swap_copy(chunk):
            span = pl.ds(chunk * 128, 128)
            return to_tp(psend.at[layer, span], precv.at[layer, span], xsend.at[layer, chunk],
                         xrecv.at[layer, chunk], partner)

        def first_half():
            conv_rows(0, 1, rows // CONV_ROWS)
            take_halo(0)
            conv_rows(0, 0, 1)
            conv_copies(0, 0, q, "start")

        advance(layer, 0, half_n)
        if layer == 0:
            pl.when(me < n - 1)(doc_copy.start)
        gate_half(0)
        pause()
        if last:
            advance(layer, 2, half_n)
            first_half()
        if layer == 0:
            advance(layer, 2, half_n)
            count_runs()
        advance(layer, 1, half_n)
        gate_half(1)
        pause()
        if not last:
            first_half()
            pause()
        for chunk in order:
            if chunk == 0:
                take_halo(1)
            conv_rows(1, 2 * chunk, 2 * chunk + 2)
            stats[layer, t, chunk] = jnp.transpose(stat[pl.ds(chunk * 128, 128), :])[:8]
            for k in range(1, m):
                stat_copy(chunk, k, t).start()
            conv_copies(1, chunk, q, "start")

        pause()
        gains = [ng_all[p, pl.ds(layer, 1), :] for p in range(pairs)]
        shifts = [ns_all[p, pl.ds(layer, 1), :] for p in range(pairs)]
        for chunk in order:
            for k in range(1, m):
                stat_copy(chunk, k, (t + k) % m).wait_recv()
            summed = stats[layer, 0, chunk]
            for who in range(1, m):
                summed = summed + stats[layer, who, chunk]
            both = jnp.transpose(jnp.concatenate([summed, jnp.zeros((120, 128), jnp.float32)], axis=0))
            row_mean = both[:, 0:1] / channels
            row_var = both[:, 1:2] / channels - row_mean * row_mean
            row_scale = lax.rsqrt(row_var + epsilon)
            if chunk == order[0]:
                conv_copies(0, 0, None, "wait_recv")
            conv_copies(1, chunk, None, "wait_recv")
            span = pl.ds(chunk * 128, 128)
            for p in range(pairs):
                normalized = gains[p] * (conv[layer, p, span, :].astype(jnp.float32) - row_mean) * row_scale + shifts[p]
                act[span, pl.ds(p * block, block)] = jax.nn.silu(normalized).astype(jnp.bfloat16)
            if chunk == order[0]:
                for k in range(1, pairs):
                    peer = (q + k) % pairs
                    part = oall.at[layer, pl.ds(pl.multiple_of(peer * block, block), block)]
                    to_tp(part, part, osend.at[layer, k], orecv.at[layer, peer], t).wait_recv()
            psend[layer, span, :] = jnp.dot(
                act[span, :], oall[layer], preferred_element_type=jnp.float32).astype(jnp.bfloat16)
            swap_copy(chunk).start()
            if chunk == order[0]:
                pause()

        pause()
        if last:
            for each in range(layers):
                drain(each)
            for copy in gain_copies:
                copy.wait_send()
            pl.when(me < n - 1)(doc_copy.wait_send)
        for chunk in order:
            swap_copy(chunk).wait_recv()

            @pl.loop(0, 128 // 32)
            def _(i, chunk=chunk):
                span = pl.ds(pl.multiple_of(chunk * 128 + i * 32, 32), 32)
                branch = (psend[layer, span, :].astype(jnp.float32)
                          + precv[layer, span, :].astype(jnp.float32)).astype(jnp.bfloat16)
                total = (source[span, :].astype(jnp.float32) + branch.astype(jnp.float32)).astype(jnp.bfloat16)
                target[span, :] = total
                if not last:
                    wide = total.astype(jnp.float32)
                    scale = lax.rsqrt(jnp.mean(wide * wide, axis=-1, keepdims=True) + epsilon)
                    normed[span, :] = (wide * scale * gain_ref[pl.ds(layer + 1, 1), :]).astype(jnp.bfloat16)

        for chunk in range(chunks):
            for k in range(1, m):
                stat_copy(chunk, k, t).wait_send()
            conv_copies(1, chunk, q, "wait_send")
            swap_copy(chunk).wait_send()
        conv_copies(0, 0, q, "wait_send")
        for kind in range(2):
            pl.when(me < n - 1)(lambda kind=kind: halo_copy(kind).wait_send())

    for layer in range(layers):
        layer_step(layer, tok_ref if layer == 0 else hid.at[layer - 1],
                   out_ref if layer + 1 == layers else hid.at[layer])


def fused_on_device(n, m, tokens, doc_ids, pre_gain, value_proj, gate_proj, out_proj, conv_taps, norm_gain, norm_shift):
    rows, width = tokens.shape
    layers, depth, block = value_proj.shape
    owidth = out_proj.shape[2]
    reach = conv_taps.shape[1] - 1
    pairs, chunks = m // 2, rows // 128
    docs = doc_ids.reshape(rows // 128, 128)
    bf16, f32, i32 = jnp.bfloat16, jnp.float32, jnp.int32
    dma = pltpu.SemaphoreType.DMA
    vmem = pl.BlockSpec(memory_space=pltpu.VMEM)
    hbm = pl.BlockSpec(memory_space=pltpu.HBM)
    return pl.pallas_call(
        functools.partial(fused_kernel, n, m, reach, layers),
        out_shape=pltpu.VMEM((rows, width), bf16),
        in_specs=[hbm] * 9,
        out_specs=vmem,
        scratch_shapes=[
            pltpu.VMEM((rows, width), bf16), pltpu.VMEM(docs.shape, i32), pltpu.VMEM(pre_gain.shape, f32),
            pltpu.VMEM(value_proj.shape, bf16), pltpu.VMEM(gate_proj.shape, bf16), pltpu.VMEM(out_proj.shape, bf16),
            pltpu.VMEM((reach + 1, layers, block), f32), pltpu.VMEM(norm_gain.shape, f32), pltpu.VMEM(norm_shift.shape, f32),
            pltpu.VMEM((layers, 2, n * depth, block), bf16),
            pltpu.VMEM((layers, pairs * block, n * owidth), bf16),
            pltpu.VMEM((rows, width), bf16),
            pltpu.VMEM((rows, block), f32),
            pltpu.VMEM((2, rows + HALO, block // 2), f32),
            pltpu.VMEM((rows + HALO, 128), f32),
            pltpu.VMEM((rows, 128), i32),
            pltpu.VMEM((layers, 2, HALO, block // 2), bf16),
            pltpu.VMEM((layers, 2, HALO, block // 2), bf16),
            pltpu.VMEM((HALO, 128), f32),
            pltpu.VMEM((HALO, 128), f32),
            pltpu.VMEM((rows, 128), f32),
            pltpu.VMEM((layers, m, chunks, 8, 128), f32),
            pltpu.VMEM((pairs, layers, block), f32),
            pltpu.VMEM((pairs, layers, block), f32),
            pltpu.VMEM((layers, pairs, rows, block), bf16),
            pltpu.VMEM((rows, pairs * block), bf16),
            pltpu.VMEM((layers, rows, width), bf16),
            pltpu.VMEM((layers, rows, width), bf16),
            pltpu.VMEM((max(1, layers - 1), rows, width), bf16),
            dma((layers, 3)), dma((layers, 3, 2, n // 2, 2)),
            dma((layers, pairs)), dma((layers, pairs)),
            dma((2 * layers + 1,)), dma((2 * layers + 1,)),
            dma((layers, m, chunks)), dma((layers, m, chunks)),
            dma((layers, pairs, chunks + 1)), dma((layers, pairs, chunks + 1)),
            dma((layers, chunks)), dma((layers, chunks)),
            dma((pairs, 2)), dma((pairs, 2)), dma((9,)),
        ],
        compiler_params=pltpu.CompilerParams(
            collective_id=0, has_side_effects=True, vmem_limit_bytes=60 * 1024 * 1024),
    )(tokens, docs, pre_gain, value_proj, gate_proj, out_proj, jnp.transpose(conv_taps, (1, 0, 2)), norm_gain, norm_shift)


def passed_along(value, axis, steps):
    count = lax.axis_size(axis)
    first, last = (max(0, -steps), min(count, count - steps))
    return lax.ppermute(value, axis, [(source, source + steps) for source in range(first, last)])


def on_device(
    tokens, doc_ids, pre_gain, value_proj, gate_proj, out_proj, conv_taps, norm_gain, norm_shift
):
    layer_count = value_proj.shape[0]
    tap_count = conv_taps.shape[1]
    reach_rows = tap_count - 1
    row_count = tokens.shape[0]
    block_width = conv_taps.shape[2]
    channels = block_width * lax.axis_size("tp")
    hidden = tokens
    full_value, full_gate, full_out = (
        lax.all_gather(value_proj, "sp", axis=1, tiled=True),
        lax.all_gather(gate_proj, "sp", axis=1, tiled=True),
        lax.all_gather(out_proj, "sp", axis=2, tiled=True),
    )
    for layer_index in range(layer_count):
        wide_state = hidden.astype(jnp.float32)
        scale = lax.rsqrt(jnp.mean(wide_state * wide_state, axis=-1, keepdims=True) + epsilon)
        normed = (wide_state * scale * pre_gain[layer_index]).astype(jnp.bfloat16)
        value_acc = jnp.dot(normed, full_value[layer_index], preferred_element_type=jnp.float32)
        gate_acc = jnp.dot(normed, full_gate[layer_index], preferred_element_type=jnp.float32)
        value_half = value_acc.astype(jnp.bfloat16)
        gate_half = gate_acc.astype(jnp.bfloat16)
        gated_rows = (
            value_half.astype(jnp.float32) * jax.nn.sigmoid(gate_half.astype(jnp.float32))
        ).astype(jnp.bfloat16)
        prev_rows, prev_docs = passed_along(
            (gated_rows[row_count - reach_rows :], doc_ids[row_count - reach_rows :]), "sp", 1
        )
        padded = jnp.concatenate([prev_rows, gated_rows]).astype(jnp.float32)
        padded_docs = jnp.concatenate([prev_docs, doc_ids])
        conv_out = jnp.zeros((row_count, block_width), jnp.float32)
        for offset in range(tap_count):
            first_row = reach_rows - offset
            same_doc = (padded_docs[first_row : first_row + row_count] == doc_ids)[:, None]
            term = (
                conv_taps[layer_index, offset][None, :] * padded[first_row : first_row + row_count]
            )
            conv_out = conv_out + jnp.where(same_doc, term, jnp.float32(0.0))
        row_sums, square_sums = lax.psum(
            (jnp.sum(conv_out, axis=1), jnp.sum(conv_out * conv_out, axis=1)), "tp"
        )
        row_mean = (row_sums / channels)[:, None]
        row_var = (square_sums / channels)[:, None] - row_mean * row_mean
        normalized = (
            norm_gain[layer_index] * (conv_out - row_mean) * lax.rsqrt(row_var + epsilon)
            + norm_shift[layer_index]
        )
        activated = jax.nn.silu(normalized).astype(jnp.bfloat16)
        partial_value = jnp.dot(
            activated, full_out[layer_index], preferred_element_type=jnp.float32
        )
        summed = lax.psum(partial_value.astype(jnp.bfloat16), "tp")
        hidden = (hidden.astype(jnp.float32) + summed.astype(jnp.float32)).astype(jnp.bfloat16)
    return hidden


def suits_kernel(n, m, tokens, value_proj, out_proj, conv_taps):
    rows, width = tokens.shape
    depth, block = value_proj.shape[1:]
    return (
        n % 2 == 0 and 4 <= n <= 16 and m % 2 == 0 and m >= 4 and rows % 128 == 0 and width % 256 == 0
        and depth % 32 == 0 and block == 256 and out_proj.shape[2] % 256 == 0
        and conv_taps.shape[1] - 1 <= HALO
    )


def solution(mesh):
    n, m = mesh.shape["sp"], mesh.shape["tp"]

    def body(tokens, doc_ids, pre_gain, value_proj, gate_proj, out_proj, conv_taps, norm_gain, norm_shift):
        chosen = on_device
        if suits_kernel(n, m, tokens, value_proj, out_proj, conv_taps):
            chosen = functools.partial(fused_on_device, n, m)
        return chosen(tokens, doc_ids, pre_gain, value_proj, gate_proj, out_proj, conv_taps, norm_gain, norm_shift)

    return jax.shard_map(
        body,
        mesh=mesh,
        in_specs=(
            P("sp", None),
            P("sp"),
            P(),
            P(None, "sp", "tp"),
            P(None, "sp", "tp"),
            P(None, "tp", "sp"),
            P(None, None, "tp"),
            P(None, "tp"),
            P(None, "tp"),
        ),
        out_specs=P("sp", None),
        check_vma=False,
    )
```

```python
import functools
import jax
import jax.numpy as jnp
from jax import lax
from jax.experimental import pallas as pl
from jax.experimental.pallas import tpu as pltpu
from jax.sharding import PartitionSpec as P

epsilon = 1e-06
MESH = pl.DeviceIdType.MESH
HALO = 32
CONV_ROWS = 64
GATE_ROWS = 64
MARKS = [2, 1, 1, 1, 1, 1, 1]


def fused_kernel(
    n, m, reach, layers,
    tok_hbm, doc_hbm, gain_hbm, v_hbm, g_hbm, o_hbm, tap_hbm, ng_hbm, ns_hbm,
    out_ref, tok_ref, doc_ref, gain_ref, v_ref, g_ref, o_ref, tap_ref, ng_ref, ns_ref,
    w, oall, normed, acc, padded, pdoc, run, ghalo, halo_in, doc_in, doc_tail,
    stat, stats, scales, conv, act, psend, precv, hid,
    rsend, rrecv, osend, orecv, hsend, hrecv, ssend, srecv, csend, crecv, xsend, xrecv, gsend, grecv, lsem,
):
    me = lax.axis_index("sp")
    t = lax.axis_index("tp")
    q, c = t // 2, t % 2
    pairs = m // 2
    half_n = n // 2
    rows, width = tok_ref.shape
    depth, block = v_ref.shape[1], v_ref.shape[2]
    owidth = o_ref.shape[2]
    hb, ho = block // 2, owidth // 2
    channels = block * m

    def index_of(position):
        position = (position + 2 * n) % n
        return jnp.where(position < half_n, 2 * position, 2 * (n - 1 - position) + 1)

    my_pos = jnp.where(me % 2 == 0, me // 2, n - 1 - me // 2)
    right, left = index_of(my_pos + 1), index_of(my_pos - 1)
    following = (me + 1) % n

    barrier = pltpu.get_barrier_semaphore()
    for other in (right, left):
        pl.semaphore_signal(barrier, inc=1, device_id={"sp": other}, device_id_type=MESH)
    for k in range(1, m):
        pl.semaphore_signal(barrier, inc=1, device_id={"tp": (t + k) % m}, device_id_type=MESH)
    loads = [pltpu.make_async_copy(src, dst, lsem.at[index]) for index, (src, dst) in enumerate(
        ((v_hbm, v_ref), (g_hbm, g_ref), (o_hbm, o_ref), (ng_hbm, ng_ref), (ns_hbm, ns_ref),
         (tok_hbm, tok_ref), (gain_hbm, gain_ref), (doc_hbm, doc_ref), (tap_hbm, tap_ref)))]
    for load in loads:
        load.start()
    pl.semaphore_wait(barrier, 1 + m)

    def to_sp(src, dst, send, recv, target):
        return pltpu.make_async_remote_copy(
            src_ref=src, dst_ref=dst, send_sem=send, recv_sem=recv,
            device_id={"sp": target}, device_id_type=MESH)

    def to_tp(src, dst, send, recv, target):
        return pltpu.make_async_remote_copy(
            src_ref=src, dst_ref=dst, send_sem=send, recv_sem=recv,
            device_id={"tp": target}, device_id_type=MESH)

    def owner_at(way, distance):
        return index_of(my_pos - distance if way == 0 else my_pos + distance)

    def held(layer, kind, owner, first=0, count=2):
        if kind < 2:
            return w.at[layer, kind, pl.ds(pl.multiple_of(owner * depth, depth), depth), pl.ds(first * hb, count * hb)]
        return oall.at[layer, pl.ds(pl.multiple_of(q * block, block), block),
                       pl.ds(pl.multiple_of(owner * owidth + first * ho, ho), count * ho)]

    def several(layer, kind, count):
        if kind < 2:
            return w.at[layer, kind, pl.ds(0, count * depth)]
        return oall.at[layer, pl.ds(pl.multiple_of(q * block, block), block), pl.ds(0, count * owidth)]

    def ring_copy(layer, kind, way, step, src, dst):
        return to_sp(src, dst, rsend.at[layer, kind], rrecv.at[layer, kind, step], right if way == 0 else left)

    def spread_copy(layer, k, src, dst):
        return to_tp(src, dst, osend.at[layer, k], orecv.at[layer, q], 2 * ((q + k) % pairs) + c)

    def advance_one(layer, kind, step):
        if step > 0:
            landed = several(layer, kind, 2 if step < half_n else 1)
            ring_copy(layer, kind, 0, step - 1, landed, landed).wait_recv()
        for way in range(2):
            owner = owner_at(way, step)
            first, count = (0, 2) if step < half_n - 1 else (way, 1)
            if step == half_n:
                continue
            dst = held(layer, kind, owner, first, count)
            if step > 0:
                ring_copy(layer, kind, way, step, dst, dst).start()
            elif kind == 2:
                ring_copy(layer, kind, way, step, o_ref.at[layer, :, pl.ds(first * ho, count * ho)], dst).start()
            else:
                for piece in range(first, first + count):
                    ring_copy(layer, kind, way, step, (v_ref, g_ref)[piece].at[layer, :, pl.ds(kind * hb, hb)],
                              held(layer, kind, owner, piece, 1)).start()
        if kind == 2 and step > 0:
            for way in range(2 if step < half_n else 1):
                for k in range(1, pairs):
                    part = held(layer, 2, owner_at(way, step))
                    spread_copy(layer, k, part, part).start()

    entries = []
    for layer in range(layers):
        for step in range(half_n + 1):
            for kind, (first, base, pace) in enumerate(
                    ((12.2, 11.7, 3.2), (12.3, 12.7, 3.2), (10.5, 11.2, 2.9)) if layer
                    else ((0, 0, 3), (1, 1, 3), (0.5, 0.5, 3))):
                shift = 11.5 * max(layer - 1, 0)
                entries.append((shift + (base + pace * step if step else first), layer, kind, step))
    pending = [entry[1:] for entry in sorted(entries)]

    def tend(count):
        for _ in range(count):
            if pending:
                advance_one(*pending.pop(0))

    def advance(*target):
        while target in pending:
            advance_one(*pending.pop(0))

    def drain(layer):
        for kind in range(3):
            ref = several(layer, kind, n - 1)
            ring_copy(layer, kind, 0, 0, ref, ref).wait_send()
        for k in range(1, pairs):
            ref = several(layer, 2, n)
            spread_copy(layer, k, ref, ref).wait_send()

    def keep_own(layer):
        row = pl.ds(pl.multiple_of(me * depth, depth), depth)
        for kind in range(2):
            w[layer, kind, row, pl.ds(0, hb)] = v_ref[layer, :, kind * hb:(kind + 1) * hb]
            w[layer, kind, row, pl.ds(hb, hb)] = g_ref[layer, :, kind * hb:(kind + 1) * hb]
        oall[layer, pl.ds(pl.multiple_of(q * block, block), block),
             pl.ds(pl.multiple_of(me * owidth, owidth), owidth)] = o_ref[layer]

    for load in loads[:5]:
        load.wait()
    tend(3)
    for layer in range(layers):
        for k in range(1, pairs):
            spread_copy(layer, k, o_ref.at[layer], held(layer, 2, me)).start()
    gain_copies = []
    for k in range(1, pairs):
        for index, src in enumerate((ng_ref, ns_ref)):
            to_tp(src, scales.at[q, index], gsend.at[k], grecv.at[q], 2 * ((q + k) % pairs) + c).start()
        gain_copies.append(to_tp(scales.at[q], scales.at[q], gsend.at[k], grecv.at[q], 2 * ((q + k) % pairs) + c))
    scales[q, 0] = ng_ref[...]
    scales[q, 1] = ns_ref[...]

    for load in loads[5:]:
        load.wait()

    def doc_block(i):
        row = doc_ref[pl.ds(i, 1), :].astype(jnp.float32)
        return jnp.transpose(jnp.broadcast_to(row, (128, 128)))

    doc_tail[...] = doc_block(rows // 128 - 1)[128 - HALO:]
    doc_copy = to_sp(doc_tail, doc_in, hsend.at[2 * layers], hrecv.at[2 * layers], following)

    for i in range(rows // 128):
        pdoc[pl.ds(HALO + i * 128, 128), :] = doc_block(i)
    pdoc[pl.ds(0, HALO), :] = jnp.full((HALO, 128), -1.0, jnp.float32)

    def norm_rows(layer, source):
        @pl.loop(0, rows // 32)
        def _(i):
            span = pl.ds(pl.multiple_of(i * 32, 32), 32)
            wide = source[span, :].astype(jnp.float32)
            scale = lax.rsqrt(jnp.mean(wide * wide, axis=-1, keepdims=True) + epsilon)
            normed[span, :] = (wide * scale * gain_ref[pl.ds(layer, 1), :]).astype(jnp.bfloat16)

    norm_rows(0, tok_ref)
    for layer in range(layers):
        keep_own(layer)

    @pl.when(me == 0)
    def _():
        halo_in[...] = jnp.zeros(halo_in.shape, halo_in.dtype)


    def count_runs():
        for k in range(1, pairs):
            peer = (q + k) % pairs
            to_tp(scales.at[peer], scales.at[peer], gsend.at[k], grecv.at[peer], 2 * peer + c).wait_recv()

        @pl.when(me > 0)
        def _():
            doc_copy.wait_recv()
            pdoc[pl.ds(0, HALO), :] = doc_in[...]

        @pl.loop(0, rows // CONV_ROWS)
        def _(i):
            base = pl.multiple_of(i * CONV_ROWS, CONV_ROWS)
            mine = pdoc[pl.ds(base + HALO, CONV_ROWS), :]
            count = jnp.zeros((CONV_ROWS, 128), jnp.int32)
            for j in range(1, reach + 1):
                count = count + (pdoc[pl.ds(base + (HALO - j), CONV_ROWS), :] == mine).astype(jnp.int32)
            run[pl.ds(base, CONV_ROWS), :] = count

    lane = lax.broadcasted_iota(jnp.int32, (CONV_ROWS, 128), 1)
    chunks = rows // 128
    order = list(range(1, chunks)) + [0]
    partner = 2 * q + 1 - c

    def layer_step(layer, source, target):
        last = layer + 1 == layers
        marks = MARKS[:]

        def pause():
            if not last and marks:
                tend(marks.pop(0))

        def halo_copy(kind):
            return to_sp(ghalo.at[layer, kind], halo_in.at[layer, kind],
                         hsend.at[2 * layer + kind], hrecv.at[2 * layer + kind], following)

        def gate_half(kind):
            acc[...] = jnp.dot(normed[...], w[layer, kind], preferred_element_type=jnp.float32)

            def gate_rows(start):
                span = pl.ds(start, GATE_ROWS)
                value = acc[span, pl.ds(0, hb)].astype(jnp.bfloat16).astype(jnp.float32)
                gate = acc[span, pl.ds(hb, hb)].astype(jnp.bfloat16).astype(jnp.float32)
                gated = (value * jax.nn.sigmoid(gate)).astype(jnp.bfloat16)
                padded[kind, pl.ds(start + HALO, GATE_ROWS), :] = gated.astype(jnp.float32)
                return gated

            ghalo[layer, kind] = gate_rows(rows - GATE_ROWS)[GATE_ROWS - HALO:]
            pl.when(me < n - 1)(lambda: halo_copy(kind).start())

            for i in range(rows // GATE_ROWS - 1):
                gate_rows(i * GATE_ROWS)

        def take_halo(kind):
            pl.when(me > 0)(lambda: halo_copy(kind).wait_recv())
            padded[kind, pl.ds(0, HALO), :] = halo_in[layer, kind].astype(jnp.float32)

        def conv_rows(kind, first, end):
            cols = pl.ds(kind * hb, hb)

            for i in range(first, end):
                base = i * CONV_ROWS
                span = pl.ds(base, CONV_ROWS)
                count = run[span, :]
                total = tap_ref[0, pl.ds(layer, 1), cols] * padded[kind, pl.ds(base + HALO, CONV_ROWS), :]
                for j in range(1, reach + 1):
                    term = tap_ref[j, pl.ds(layer, 1), cols] * padded[kind, pl.ds(base + (HALO - j), CONV_ROWS), :]
                    total = total + jnp.where(count >= j, term, jnp.float32(0.0))
                conv[layer, q, span, cols] = total.astype(jnp.bfloat16)
                sums = jnp.where(
                    lane == 0, jnp.sum(total, axis=1, keepdims=True),
                    jnp.where(lane == 1, jnp.sum(total * total, axis=1, keepdims=True), jnp.float32(0.0)))
                if kind:
                    sums = sums + stat[span, :]
                stat[span, :] = sums

        def conv_copies(kind, chunk):
            part = conv.at[layer, q, pl.ds(chunk * 128, 128), pl.ds(kind * hb, hb)]
            for k in range(1, pairs):
                to_tp(part, part, csend.at[layer], crecv.at[layer, chunk], 2 * ((q + k) % pairs) + c).start()

        def conv_landed(chunk):
            part = conv.at[layer, pl.ds(0, pairs - 1), pl.ds(chunk * 128, 128)]
            return to_tp(part, part, csend.at[layer], crecv.at[layer, chunk], partner)

        def stat_copies(chunk):
            part = stats.at[layer, chunk, t]
            for k in range(1, m):
                to_tp(part, part, ssend.at[layer], srecv.at[layer, chunk], (t + k) % m).start()

        def stats_landed(chunk):
            part = stats.at[layer, chunk, pl.ds(0, m - 1)]
            return to_tp(part, part, ssend.at[layer], srecv.at[layer, chunk], partner)

        def swap_copy(chunk):
            span = pl.ds(chunk * 128, 128)
            return to_tp(psend.at[layer, span], precv.at[layer, span], xsend.at[layer],
                         xrecv.at[layer, chunk], partner)

        def first_rows(chunk):
            conv_rows(0, 2 * chunk, 2 * chunk + 2)
            conv_copies(0, chunk)

        advance(layer, 0, half_n)
        if layer == 0:
            pl.when(me < n - 1)(doc_copy.start)
        gate_half(0)
        if layer == 0:
            advance(layer, 2, half_n)
            pause()
            count_runs()
        if last:
            for chunk in order[:-1]:
                first_rows(chunk)
        advance(layer, 1, half_n)
        gate_half(1)
        if not last:
            pause()
            for chunk in order[:-1]:
                first_rows(chunk)
        for chunk in order:
            if chunk == 0:
                take_halo(0)
                first_rows(0)
                pause()
                take_halo(1)
            conv_rows(1, 2 * chunk, 2 * chunk + 2)
            stats[layer, chunk, t] = jnp.transpose(stat[pl.ds(chunk * 128, 128), :])[:8]
            stat_copies(chunk)
            conv_copies(1, chunk)

        pause()
        gains = [scales[p, 0, pl.ds(layer, 1), :] for p in range(pairs)]
        shifts = [scales[p, 1, pl.ds(layer, 1), :] for p in range(pairs)]
        for chunk in order:
            stats_landed(chunk).wait_recv()
            summed = stats[layer, chunk, 0]
            for who in range(1, m):
                summed = summed + stats[layer, chunk, who]
            both = jnp.transpose(jnp.concatenate([summed, jnp.zeros((120, 128), jnp.float32)], axis=0))
            row_mean = both[:, 0:1] / channels
            row_var = both[:, 1:2] / channels - row_mean * row_mean
            row_scale = lax.rsqrt(row_var + epsilon)
            conv_landed(chunk).wait_recv()
            span = pl.ds(chunk * 128, 128)
            for p in range(pairs):
                normalized = gains[p] * (conv[layer, p, span, :].astype(jnp.float32) - row_mean) * row_scale + shifts[p]
                act[span, pl.ds(p * block, block)] = jax.nn.silu(normalized).astype(jnp.bfloat16)
            if chunk == order[0]:
                advance(layer, 2, half_n)
                for k in range(1, pairs):
                    peer = (q + k) % pairs
                    part = oall.at[layer, pl.ds(pl.multiple_of(peer * block, block), block)]
                    to_tp(part, part, osend.at[layer, k], orecv.at[layer, peer], t).wait_recv()
            psend[layer, span, :] = jnp.dot(
                act[span, :], oall[layer], preferred_element_type=jnp.float32).astype(jnp.bfloat16)
            swap_copy(chunk).start()
            if chunk == order[0]:
                pause()

        pause()
        if last:
            for each in range(layers):
                drain(each)
            for copy in gain_copies:
                copy.wait_send()
            pl.when(me < n - 1)(doc_copy.wait_send)
        for chunk in order:
            swap_copy(chunk).wait_recv()

            @pl.loop(0, 128 // 32, unroll=True)
            def _(i, chunk=chunk):
                span = pl.ds(pl.multiple_of(chunk * 128 + i * 32, 32), 32)
                branch = (psend[layer, span, :].astype(jnp.float32)
                          + precv[layer, span, :].astype(jnp.float32)).astype(jnp.bfloat16)
                total = (source[span, :].astype(jnp.float32) + branch.astype(jnp.float32)).astype(jnp.bfloat16)
                target[span, :] = total
                if not last:
                    wide = total.astype(jnp.float32)
                    scale = lax.rsqrt(jnp.mean(wide * wide, axis=-1, keepdims=True) + epsilon)
                    normed[span, :] = (wide * scale * gain_ref[pl.ds(layer + 1, 1), :]).astype(jnp.bfloat16)

        for refs, sem in ((stats.at[layer, :, pl.ds(0, m - 1)], ssend), (conv.at[layer, pl.ds(0, pairs - 1)], csend),
                          (psend.at[layer], xsend)):
            to_tp(refs, refs, sem.at[layer], xrecv.at[layer, 0], partner).wait_send()
        for kind in range(2):
            pl.when(me < n - 1)(lambda kind=kind: halo_copy(kind).wait_send())

    for layer in range(layers):
        layer_step(layer, tok_ref if layer == 0 else hid.at[layer - 1],
                   out_ref if layer + 1 == layers else hid.at[layer])


def fused_on_device(n, m, tokens, doc_ids, pre_gain, value_proj, gate_proj, out_proj, conv_taps, norm_gain, norm_shift):
    rows, width = tokens.shape
    layers, depth, block = value_proj.shape
    owidth = out_proj.shape[2]
    reach = conv_taps.shape[1] - 1
    pairs, chunks = m // 2, rows // 128
    docs = doc_ids.reshape(rows // 128, 128)
    bf16, f32, i32 = jnp.bfloat16, jnp.float32, jnp.int32
    dma = pltpu.SemaphoreType.DMA
    vmem = pl.BlockSpec(memory_space=pltpu.VMEM)
    hbm = pl.BlockSpec(memory_space=pltpu.HBM)
    return pl.pallas_call(
        functools.partial(fused_kernel, n, m, reach, layers),
        out_shape=pltpu.VMEM((rows, width), bf16),
        in_specs=[hbm] * 9,
        out_specs=vmem,
        scratch_shapes=[
            pltpu.VMEM((rows, width), bf16), pltpu.VMEM(docs.shape, i32), pltpu.VMEM(pre_gain.shape, f32),
            pltpu.VMEM(value_proj.shape, bf16), pltpu.VMEM(gate_proj.shape, bf16), pltpu.VMEM(out_proj.shape, bf16),
            pltpu.VMEM((reach + 1, layers, block), f32), pltpu.VMEM(norm_gain.shape, f32), pltpu.VMEM(norm_shift.shape, f32),
            pltpu.VMEM((layers, 2, n * depth, block), bf16),
            pltpu.VMEM((layers, pairs * block, n * owidth), bf16),
            pltpu.VMEM((rows, width), bf16),
            pltpu.VMEM((rows, block), f32),
            pltpu.VMEM((2, rows + HALO, block // 2), f32),
            pltpu.VMEM((rows + HALO, 128), f32),
            pltpu.VMEM((rows, 128), i32),
            pltpu.VMEM((layers, 2, HALO, block // 2), bf16),
            pltpu.VMEM((layers, 2, HALO, block // 2), bf16),
            pltpu.VMEM((HALO, 128), f32),
            pltpu.VMEM((HALO, 128), f32),
            pltpu.VMEM((rows, 128), f32),
            pltpu.VMEM((layers, chunks, m, 8, 128), f32),
            pltpu.VMEM((pairs, 2, layers, block), f32),
            pltpu.VMEM((layers, pairs, rows, block), bf16),
            pltpu.VMEM((rows, pairs * block), bf16),
            pltpu.VMEM((layers, rows, width), bf16),
            pltpu.VMEM((layers, rows, width), bf16),
            pltpu.VMEM((max(1, layers - 1), rows, width), bf16),
            dma((layers, 3)), dma((layers, 3, n // 2)),
            dma((layers, pairs)), dma((layers, pairs)),
            dma((2 * layers + 1,)), dma((2 * layers + 1,)),
            dma((layers,)), dma((layers, chunks)),
            dma((layers,)), dma((layers, chunks)),
            dma((layers,)), dma((layers, chunks)),
            dma((pairs,)), dma((pairs,)), dma((9,)),
        ],
        compiler_params=pltpu.CompilerParams(
            collective_id=0, has_side_effects=True, vmem_limit_bytes=60 * 1024 * 1024),
    )(tokens, docs, pre_gain, value_proj, gate_proj, out_proj, jnp.transpose(conv_taps, (1, 0, 2)), norm_gain, norm_shift)


def passed_along(value, axis, steps):
    count = lax.axis_size(axis)
    first, last = (max(0, -steps), min(count, count - steps))
    return lax.ppermute(value, axis, [(source, source + steps) for source in range(first, last)])


def on_device(
    tokens, doc_ids, pre_gain, value_proj, gate_proj, out_proj, conv_taps, norm_gain, norm_shift
):
    layer_count = value_proj.shape[0]
    tap_count = conv_taps.shape[1]
    reach_rows = tap_count - 1
    row_count = tokens.shape[0]
    block_width = conv_taps.shape[2]
    channels = block_width * lax.axis_size("tp")
    hidden = tokens
    full_value, full_gate, full_out = (
        lax.all_gather(value_proj, "sp", axis=1, tiled=True),
        lax.all_gather(gate_proj, "sp", axis=1, tiled=True),
        lax.all_gather(out_proj, "sp", axis=2, tiled=True),
    )
    for layer_index in range(layer_count):
        wide_state = hidden.astype(jnp.float32)
        scale = lax.rsqrt(jnp.mean(wide_state * wide_state, axis=-1, keepdims=True) + epsilon)
        normed = (wide_state * scale * pre_gain[layer_index]).astype(jnp.bfloat16)
        value_acc = jnp.dot(normed, full_value[layer_index], preferred_element_type=jnp.float32)
        gate_acc = jnp.dot(normed, full_gate[layer_index], preferred_element_type=jnp.float32)
        value_half = value_acc.astype(jnp.bfloat16)
        gate_half = gate_acc.astype(jnp.bfloat16)
        gated_rows = (
            value_half.astype(jnp.float32) * jax.nn.sigmoid(gate_half.astype(jnp.float32))
        ).astype(jnp.bfloat16)
        prev_rows, prev_docs = passed_along(
            (gated_rows[row_count - reach_rows :], doc_ids[row_count - reach_rows :]), "sp", 1
        )
        padded = jnp.concatenate([prev_rows, gated_rows]).astype(jnp.float32)
        padded_docs = jnp.concatenate([prev_docs, doc_ids])
        conv_out = jnp.zeros((row_count, block_width), jnp.float32)
        for offset in range(tap_count):
            first_row = reach_rows - offset
            same_doc = (padded_docs[first_row : first_row + row_count] == doc_ids)[:, None]
            term = (
                conv_taps[layer_index, offset][None, :] * padded[first_row : first_row + row_count]
            )
            conv_out = conv_out + jnp.where(same_doc, term, jnp.float32(0.0))
        row_sums, square_sums = lax.psum(
            (jnp.sum(conv_out, axis=1), jnp.sum(conv_out * conv_out, axis=1)), "tp"
        )
        row_mean = (row_sums / channels)[:, None]
        row_var = (square_sums / channels)[:, None] - row_mean * row_mean
        normalized = (
            norm_gain[layer_index] * (conv_out - row_mean) * lax.rsqrt(row_var + epsilon)
            + norm_shift[layer_index]
        )
        activated = jax.nn.silu(normalized).astype(jnp.bfloat16)
        partial_value = jnp.dot(
            activated, full_out[layer_index], preferred_element_type=jnp.float32
        )
        summed = lax.psum(partial_value.astype(jnp.bfloat16), "tp")
        hidden = (hidden.astype(jnp.float32) + summed.astype(jnp.float32)).astype(jnp.bfloat16)
    return hidden


def suits_kernel(n, m, tokens, value_proj, out_proj, conv_taps):
    rows, width = tokens.shape
    depth, block = value_proj.shape[1:]
    return (
        n % 2 == 0 and 4 <= n <= 16 and HALO <= GATE_ROWS and m % 2 == 0 and m >= 4 and rows % 128 == 0 and width % 256 == 0
        and depth % 32 == 0 and block == 256 and out_proj.shape[2] % 256 == 0
        and conv_taps.shape[1] - 1 <= HALO
    )


def solution(mesh):
    n, m = mesh.shape["sp"], mesh.shape["tp"]

    def body(tokens, doc_ids, pre_gain, value_proj, gate_proj, out_proj, conv_taps, norm_gain, norm_shift):
        chosen = on_device
        if suits_kernel(n, m, tokens, value_proj, out_proj, conv_taps):
            chosen = functools.partial(fused_on_device, n, m)
        return chosen(tokens, doc_ids, pre_gain, value_proj, gate_proj, out_proj, conv_taps, norm_gain, norm_shift)

    return jax.shard_map(
        body,
        mesh=mesh,
        in_specs=(
            P("sp", None),
            P("sp"),
            P(),
            P(None, "sp", "tp"),
            P(None, "sp", "tp"),
            P(None, "tp", "sp"),
            P(None, None, "tp"),
            P(None, "tp"),
            P(None, "tp"),
        ),
        out_specs=P("sp", None),
        check_vma=False,
    )
```

```python
import functools
import jax
import jax.numpy as jnp
from jax import lax
from jax.experimental import pallas as pl
from jax.experimental.pallas import tpu as pltpu
from jax.sharding import PartitionSpec as P

epsilon = 1e-06
MESH = pl.DeviceIdType.MESH
HALO = 32
CONV_ROWS = 64
GATE_ROWS = 64
MARKS = [2, 1, 1, 1, 1, 1, 1]


def fused_kernel(
    n, m, reach, layers,
    tok_hbm, doc_hbm, gain_hbm, v_hbm, g_hbm, o_hbm, tap_hbm, ng_hbm, ns_hbm,
    out_ref, tok_ref, doc_ref, gain_ref, v_ref, g_ref, o_ref, tap_ref, ng_ref, ns_ref,
    w, oall, normed, acc, padded, pdoc, run, ghalo, halo_in, doc_in, doc_tail,
    stat, stats, scales, conv, act, psend, precv, hid,
    rsend, rrecv, osend, orecv, hsend, hrecv, ssend, srecv, csend, crecv, xsend, xrecv, gsend, grecv, lsem,
):
    me = lax.axis_index("sp")
    t = lax.axis_index("tp")
    q, c = t // 2, t % 2
    pairs = m // 2
    half_n = n // 2
    rows, width = tok_ref.shape
    depth, block = v_ref.shape[1], v_ref.shape[2]
    owidth = o_ref.shape[2]
    hb, ho = block // 2, owidth // 2
    channels = block * m

    def index_of(position):
        position = (position + 2 * n) % n
        return jnp.where(position < half_n, 2 * position, 2 * (n - 1 - position) + 1)

    my_pos = jnp.where(me % 2 == 0, me // 2, n - 1 - me // 2)
    right, left = index_of(my_pos + 1), index_of(my_pos - 1)
    following = (me + 1) % n

    barrier = pltpu.get_barrier_semaphore()
    for other in (right, left):
        pl.semaphore_signal(barrier, inc=1, device_id={"sp": other}, device_id_type=MESH)
    for k in range(1, m):
        pl.semaphore_signal(barrier, inc=1, device_id={"tp": (t + k) % m}, device_id_type=MESH)
    loads = [pltpu.make_async_copy(src, dst, lsem.at[index]) for index, (src, dst) in enumerate(
        ((v_hbm, v_ref), (g_hbm, g_ref), (o_hbm, o_ref), (ng_hbm, ng_ref), (ns_hbm, ns_ref),
         (tok_hbm, tok_ref), (gain_hbm, gain_ref), (doc_hbm, doc_ref), (tap_hbm, tap_ref)))]
    for load in loads:
        load.start()
    pl.semaphore_wait(barrier, 1 + m)

    def to_sp(src, dst, send, recv, target):
        return pltpu.make_async_remote_copy(
            src_ref=src, dst_ref=dst, send_sem=send, recv_sem=recv,
            device_id={"sp": target}, device_id_type=MESH)

    def to_tp(src, dst, send, recv, target):
        return pltpu.make_async_remote_copy(
            src_ref=src, dst_ref=dst, send_sem=send, recv_sem=recv,
            device_id={"tp": target}, device_id_type=MESH)

    def owner_at(way, distance):
        return index_of(my_pos - distance if way == 0 else my_pos + distance)

    def held(layer, kind, owner, first=0, count=2):
        if kind < 2:
            return w.at[layer, kind, pl.ds(pl.multiple_of(owner * depth, depth), depth), pl.ds(first * hb, count * hb)]
        return oall.at[layer, pl.ds(pl.multiple_of(q * block, block), block),
                       pl.ds(pl.multiple_of(owner * owidth + first * ho, ho), count * ho)]

    def several(layer, kind, count):
        if kind < 2:
            return w.at[layer, kind, pl.ds(0, count * depth)]
        return oall.at[layer, pl.ds(pl.multiple_of(q * block, block), block), pl.ds(0, count * owidth)]

    def ring_copy(layer, kind, way, step, src, dst):
        return to_sp(src, dst, rsend.at[layer, kind], rrecv.at[layer, kind, step], right if way == 0 else left)

    def spread_copy(layer, k, src, dst):
        return to_tp(src, dst, osend.at[layer, k], orecv.at[layer, q], 2 * ((q + k) % pairs) + c)

    def advance_one(layer, kind, step):
        if step > 0:
            landed = several(layer, kind, 2 if step < half_n else 1)
            ring_copy(layer, kind, 0, step - 1, landed, landed).wait_recv()
        for way in range(2):
            owner = owner_at(way, step)
            first, count = (0, 2) if step < half_n - 1 else (way, 1)
            if step == half_n:
                continue
            dst = held(layer, kind, owner, first, count)
            if step > 0:
                ring_copy(layer, kind, way, step, dst, dst).start()
            elif kind == 2:
                ring_copy(layer, kind, way, step, o_ref.at[layer, :, pl.ds(first * ho, count * ho)], dst).start()
            else:
                for piece in range(first, first + count):
                    ring_copy(layer, kind, way, step, (v_ref, g_ref)[piece].at[layer, :, pl.ds(kind * hb, hb)],
                              held(layer, kind, owner, piece, 1)).start()
        if kind == 2 and step > 0:
            for way in range(2 if step < half_n else 1):
                for k in range(1, pairs):
                    part = held(layer, 2, owner_at(way, step))
                    spread_copy(layer, k, part, part).start()

    entries = []
    for layer in range(layers):
        for step in range(half_n + 1):
            for kind, (first, base, pace) in enumerate(
                    ((12.2, 11.7, 3.2), (12.3, 12.7, 3.2), (10.5, 11.2, 2.9)) if layer
                    else ((0, 0, 3), (1, 1, 3), (0.5, 0.5, 3))):
                shift = 11.5 * max(layer - 1, 0)
                entries.append((shift + (base + pace * step if step else first), layer, kind, step))
    pending = [entry[1:] for entry in sorted(entries)]

    def tend(count):
        for _ in range(count):
            if pending:
                advance_one(*pending.pop(0))

    def advance(*target):
        while target in pending:
            advance_one(*pending.pop(0))

    def drain(layer):
        for kind in range(3):
            ref = several(layer, kind, n - 1)
            ring_copy(layer, kind, 0, 0, ref, ref).wait_send()
        for k in range(1, pairs):
            ref = several(layer, 2, n)
            spread_copy(layer, k, ref, ref).wait_send()

    def keep_own(layer):
        row = pl.ds(pl.multiple_of(me * depth, depth), depth)
        for kind in range(2):
            w[layer, kind, row, pl.ds(0, hb)] = v_ref[layer, :, kind * hb:(kind + 1) * hb]
            w[layer, kind, row, pl.ds(hb, hb)] = g_ref[layer, :, kind * hb:(kind + 1) * hb]
        oall[layer, pl.ds(pl.multiple_of(q * block, block), block),
             pl.ds(pl.multiple_of(me * owidth, owidth), owidth)] = o_ref[layer]

    for load in loads[:5]:
        load.wait()
    tend(3)
    for layer in range(layers):
        for k in range(1, pairs):
            spread_copy(layer, k, o_ref.at[layer], held(layer, 2, me)).start()
    gain_copies = []
    for k in range(1, pairs):
        for index, src in enumerate((ng_ref, ns_ref)):
            to_tp(src, scales.at[q, index], gsend.at[k], grecv.at[q], 2 * ((q + k) % pairs) + c).start()
        gain_copies.append(to_tp(scales.at[q], scales.at[q], gsend.at[k], grecv.at[q], 2 * ((q + k) % pairs) + c))
    scales[q, 0] = ng_ref[...]
    scales[q, 1] = ns_ref[...]

    for load in loads[5:]:
        load.wait()

    def doc_block(i):
        row = doc_ref[pl.ds(i, 1), :].astype(jnp.float32)
        return jnp.transpose(jnp.broadcast_to(row, (128, 128)))

    doc_tail[...] = doc_block(rows // 128 - 1)[128 - HALO:]
    doc_copy = to_sp(doc_tail, doc_in, hsend.at[2 * layers], hrecv.at[2 * layers], following)

    for i in range(rows // 128):
        pdoc[pl.ds(HALO + i * 128, 128), :] = doc_block(i)
    pdoc[pl.ds(0, HALO), :] = jnp.full((HALO, 128), -1.0, jnp.float32)

    def norm_rows(layer, source):
        @pl.loop(0, rows // 32)
        def _(i):
            span = pl.ds(pl.multiple_of(i * 32, 32), 32)
            wide = source[span, :].astype(jnp.float32)
            scale = lax.rsqrt(jnp.mean(wide * wide, axis=-1, keepdims=True) + epsilon)
            normed[span, :] = (wide * scale * gain_ref[pl.ds(layer, 1), :]).astype(jnp.bfloat16)

    norm_rows(0, tok_ref)
    for layer in range(layers):
        keep_own(layer)

    @pl.when(me == 0)
    def _():
        halo_in[...] = jnp.zeros(halo_in.shape, halo_in.dtype)


    def count_runs():
        for k in range(1, pairs):
            peer = (q + k) % pairs
            to_tp(scales.at[peer], scales.at[peer], gsend.at[k], grecv.at[peer], 2 * peer + c).wait_recv()

        @pl.when(me > 0)
        def _():
            doc_copy.wait_recv()
            pdoc[pl.ds(0, HALO), :] = doc_in[...]

        @pl.loop(0, rows // CONV_ROWS)
        def _(i):
            base = pl.multiple_of(i * CONV_ROWS, CONV_ROWS)
            mine = pdoc[pl.ds(base + HALO, CONV_ROWS), :]
            count = jnp.zeros((CONV_ROWS, 128), jnp.int32)
            for j in range(1, reach + 1):
                count = count + (pdoc[pl.ds(base + (HALO - j), CONV_ROWS), :] == mine).astype(jnp.int32)
            run[pl.ds(base, CONV_ROWS), :] = count

    lane = lax.broadcasted_iota(jnp.int32, (CONV_ROWS, 128), 1)
    chunks = rows // 128
    order = list(range(1, chunks)) + [0]
    partner = 2 * q + 1 - c

    def layer_step(layer, source, target):
        last = layer + 1 == layers
        marks = MARKS[:]

        def pause():
            if not last and marks:
                tend(marks.pop(0))

        def halo_copy(kind):
            return to_sp(ghalo.at[layer, kind], halo_in.at[layer, kind],
                         hsend.at[2 * layer + kind], hrecv.at[2 * layer + kind], following)

        def gate_half(kind):
            if layer == 0:
                acc[kind] = jnp.dot(normed[...], w[layer, kind], preferred_element_type=jnp.float32)

            def gate_rows(start):
                span = pl.ds(start, GATE_ROWS)
                value = acc[kind, span, pl.ds(0, hb)].astype(jnp.bfloat16).astype(jnp.float32)
                gate = acc[kind, span, pl.ds(hb, hb)].astype(jnp.bfloat16).astype(jnp.float32)
                gated = (value * jax.nn.sigmoid(gate)).astype(jnp.bfloat16)
                padded[kind, pl.ds(start + HALO, GATE_ROWS), :] = gated.astype(jnp.float32)
                return gated

            ghalo[layer, kind] = gate_rows(rows - GATE_ROWS)[GATE_ROWS - HALO:]
            pl.when(me < n - 1)(lambda: halo_copy(kind).start())

            for i in range(rows // GATE_ROWS - 1):
                gate_rows(i * GATE_ROWS)

        def take_halo(kind):
            pl.when(me > 0)(lambda: halo_copy(kind).wait_recv())
            padded[kind, pl.ds(0, HALO), :] = halo_in[layer, kind].astype(jnp.float32)

        def conv_rows(kind, first, end):
            cols = pl.ds(kind * hb, hb)

            for i in range(first, end):
                base = i * CONV_ROWS
                span = pl.ds(base, CONV_ROWS)
                count = run[span, :]
                total = tap_ref[0, pl.ds(layer, 1), cols] * padded[kind, pl.ds(base + HALO, CONV_ROWS), :]
                for j in range(1, reach + 1):
                    term = tap_ref[j, pl.ds(layer, 1), cols] * padded[kind, pl.ds(base + (HALO - j), CONV_ROWS), :]
                    total = total + jnp.where(count >= j, term, jnp.float32(0.0))
                conv[layer, q, span, cols] = total.astype(jnp.bfloat16)
                sums = jnp.where(
                    lane == 0, jnp.sum(total, axis=1, keepdims=True),
                    jnp.where(lane == 1, jnp.sum(total * total, axis=1, keepdims=True), jnp.float32(0.0)))
                if kind:
                    sums = sums + stat[span, :]
                stat[span, :] = sums

        def conv_copies(kind, chunk):
            part = conv.at[layer, q, pl.ds(chunk * 128, 128), pl.ds(kind * hb, hb)]
            for k in range(1, pairs):
                to_tp(part, part, csend.at[layer], crecv.at[layer, chunk], 2 * ((q + k) % pairs) + c).start()

        def conv_landed(chunk):
            part = conv.at[layer, pl.ds(0, pairs - 1), pl.ds(chunk * 128, 128)]
            return to_tp(part, part, csend.at[layer], crecv.at[layer, chunk], partner)

        def stat_copies(chunk):
            part = stats.at[layer, chunk, t]
            for k in range(1, m):
                to_tp(part, part, ssend.at[layer], srecv.at[layer, chunk], (t + k) % m).start()

        def stats_landed(chunk):
            part = stats.at[layer, chunk, pl.ds(0, m - 1)]
            return to_tp(part, part, ssend.at[layer], srecv.at[layer, chunk], partner)

        def swap_copy(chunk):
            span = pl.ds(chunk * 128, 128)
            return to_tp(psend.at[layer, span], precv.at[layer, span], xsend.at[layer],
                         xrecv.at[layer, chunk], partner)

        def first_rows(chunk):
            conv_rows(0, 2 * chunk, 2 * chunk + 2)
            if not last or chunk == order[0]:
                conv_copies(0, chunk)

        def absorb(kind, step):
            for way in range(2 if 0 < step < half_n else 1):
                owner = owner_at(way, step)
                span = pl.ds(pl.multiple_of(owner * depth, depth), depth)
                part = jnp.dot(normed[:, span], w[layer, kind, span, :], preferred_element_type=jnp.float32)
                acc[kind] = acc[kind] + part if step else part

        def gather(kind):
            while (layer, kind, half_n) in pending:
                entry = pending.pop(0)
                advance_one(*entry)
                if layer and entry[0] == layer and entry[1] < 2:
                    absorb(*entry[1:])

        if layer:
            for step in range(half_n + 1):
                for kind in range(2):
                    if (layer, kind, step) not in pending:
                        absorb(kind, step)
        gather(0)
        if layer == 0:
            pl.when(me < n - 1)(doc_copy.start)
        gate_half(0)
        if layer == 0:
            advance(layer, 2, half_n)
            pause()
            count_runs()
        if last:
            for chunk in order[:-1]:
                first_rows(chunk)
        gather(1)
        gate_half(1)
        if not last:
            pause()
            for chunk in order[:-1]:
                first_rows(chunk)
        for chunk in order:
            if chunk == 0:
                conv_rows(0, 1, 2)
                conv_rows(1, 1, 2)
                take_halo(0)
                conv_rows(0, 0, 1)
                conv_copies(0, 0)
                pause()
                take_halo(1)
                conv_rows(1, 0, 1)
            else:
                conv_rows(1, 2 * chunk, 2 * chunk + 2)
            stats[layer, chunk, t] = jnp.transpose(stat[pl.ds(chunk * 128, 128), :])[:8]
            stat_copies(chunk)
            if last and chunk in order[1:-1]:
                conv_copies(0, chunk)
            conv_copies(1, chunk)

        pause()
        gains = [scales[p, 0, pl.ds(layer, 1), :] for p in range(pairs)]
        shifts = [scales[p, 1, pl.ds(layer, 1), :] for p in range(pairs)]
        for chunk in order:
            stats_landed(chunk).wait_recv()
            summed = stats[layer, chunk, 0]
            for who in range(1, m):
                summed = summed + stats[layer, chunk, who]
            both = jnp.transpose(jnp.concatenate([summed, jnp.zeros((120, 128), jnp.float32)], axis=0))
            row_mean = both[:, 0:1] / channels
            row_var = both[:, 1:2] / channels - row_mean * row_mean
            row_scale = lax.rsqrt(row_var + epsilon)
            conv_landed(chunk).wait_recv()
            span = pl.ds(chunk * 128, 128)
            for p in range(pairs):
                normalized = gains[p] * (conv[layer, p, span, :].astype(jnp.float32) - row_mean) * row_scale + shifts[p]
                act[span, pl.ds(p * block, block)] = jax.nn.silu(normalized).astype(jnp.bfloat16)
            if chunk == order[0]:
                advance(layer, 2, half_n)
                for k in range(1, pairs):
                    peer = (q + k) % pairs
                    part = oall.at[layer, pl.ds(pl.multiple_of(peer * block, block), block)]
                    to_tp(part, part, osend.at[layer, k], orecv.at[layer, peer], t).wait_recv()
            psend[layer, span, :] = jnp.dot(
                act[span, :], oall[layer], preferred_element_type=jnp.float32).astype(jnp.bfloat16)
            swap_copy(chunk).start()
            if chunk == order[0]:
                pause()

        pause()
        if last:
            for each in range(layers):
                drain(each)
            for copy in gain_copies:
                copy.wait_send()
            pl.when(me < n - 1)(doc_copy.wait_send)
        for chunk in order:
            swap_copy(chunk).wait_recv()

            @pl.loop(0, 128 // 32, unroll=True)
            def _(i, chunk=chunk):
                span = pl.ds(pl.multiple_of(chunk * 128 + i * 32, 32), 32)
                branch = (psend[layer, span, :].astype(jnp.float32)
                          + precv[layer, span, :].astype(jnp.float32)).astype(jnp.bfloat16)
                total = (source[span, :].astype(jnp.float32) + branch.astype(jnp.float32)).astype(jnp.bfloat16)
                target[span, :] = total
                if not last:
                    wide = total.astype(jnp.float32)
                    scale = lax.rsqrt(jnp.mean(wide * wide, axis=-1, keepdims=True) + epsilon)
                    normed[span, :] = (wide * scale * gain_ref[pl.ds(layer + 1, 1), :]).astype(jnp.bfloat16)

        for refs, sem in ((stats.at[layer, :, pl.ds(0, m - 1)], ssend), (conv.at[layer, pl.ds(0, pairs - 1)], csend),
                          (psend.at[layer], xsend)):
            to_tp(refs, refs, sem.at[layer], xrecv.at[layer, 0], partner).wait_send()
        for kind in range(2):
            pl.when(me < n - 1)(lambda kind=kind: halo_copy(kind).wait_send())

    for layer in range(layers):
        layer_step(layer, tok_ref if layer == 0 else hid.at[layer - 1],
                   out_ref if layer + 1 == layers else hid.at[layer])


def fused_on_device(n, m, tokens, doc_ids, pre_gain, value_proj, gate_proj, out_proj, conv_taps, norm_gain, norm_shift):
    rows, width = tokens.shape
    layers, depth, block = value_proj.shape
    owidth = out_proj.shape[2]
    reach = conv_taps.shape[1] - 1
    pairs, chunks = m // 2, rows // 128
    docs = doc_ids.reshape(rows // 128, 128)
    bf16, f32, i32 = jnp.bfloat16, jnp.float32, jnp.int32
    dma = pltpu.SemaphoreType.DMA
    vmem = pl.BlockSpec(memory_space=pltpu.VMEM)
    hbm = pl.BlockSpec(memory_space=pltpu.HBM)
    return pl.pallas_call(
        functools.partial(fused_kernel, n, m, reach, layers),
        out_shape=pltpu.VMEM((rows, width), bf16),
        in_specs=[hbm] * 9,
        out_specs=vmem,
        scratch_shapes=[
            pltpu.VMEM((rows, width), bf16), pltpu.VMEM(docs.shape, i32), pltpu.VMEM(pre_gain.shape, f32),
            pltpu.VMEM(value_proj.shape, bf16), pltpu.VMEM(gate_proj.shape, bf16), pltpu.VMEM(out_proj.shape, bf16),
            pltpu.VMEM((reach + 1, layers, block), f32), pltpu.VMEM(norm_gain.shape, f32), pltpu.VMEM(norm_shift.shape, f32),
            pltpu.VMEM((layers, 2, n * depth, block), bf16),
            pltpu.VMEM((layers, pairs * block, n * owidth), bf16),
            pltpu.VMEM((rows, width), bf16),
            pltpu.VMEM((2, rows, block), f32),
            pltpu.VMEM((2, rows + HALO, block // 2), f32),
            pltpu.VMEM((rows + HALO, 128), f32),
            pltpu.VMEM((rows, 128), i32),
            pltpu.VMEM((layers, 2, HALO, block // 2), bf16),
            pltpu.VMEM((layers, 2, HALO, block // 2), bf16),
            pltpu.VMEM((HALO, 128), f32),
            pltpu.VMEM((HALO, 128), f32),
            pltpu.VMEM((rows, 128), f32),
            pltpu.VMEM((layers, chunks, m, 8, 128), f32),
            pltpu.VMEM((pairs, 2, layers, block), f32),
            pltpu.VMEM((layers, pairs, rows, block), bf16),
            pltpu.VMEM((rows, pairs * block), bf16),
            pltpu.VMEM((layers, rows, width), bf16),
            pltpu.VMEM((layers, rows, width), bf16),
            pltpu.VMEM((max(1, layers - 1), rows, width), bf16),
            dma((layers, 3)), dma((layers, 3, n // 2)),
            dma((layers, pairs)), dma((layers, pairs)),
            dma((2 * layers + 1,)), dma((2 * layers + 1,)),
            dma((layers,)), dma((layers, chunks)),
            dma((layers,)), dma((layers, chunks)),
            dma((layers,)), dma((layers, chunks)),
            dma((pairs,)), dma((pairs,)), dma((9,)),
        ],
        compiler_params=pltpu.CompilerParams(
            collective_id=0, has_side_effects=True, vmem_limit_bytes=60 * 1024 * 1024),
    )(tokens, docs, pre_gain, value_proj, gate_proj, out_proj, jnp.transpose(conv_taps, (1, 0, 2)), norm_gain, norm_shift)


def passed_along(value, axis, steps):
    count = lax.axis_size(axis)
    first, last = (max(0, -steps), min(count, count - steps))
    return lax.ppermute(value, axis, [(source, source + steps) for source in range(first, last)])


def on_device(
    tokens, doc_ids, pre_gain, value_proj, gate_proj, out_proj, conv_taps, norm_gain, norm_shift
):
    layer_count = value_proj.shape[0]
    tap_count = conv_taps.shape[1]
    reach_rows = tap_count - 1
    row_count = tokens.shape[0]
    block_width = conv_taps.shape[2]
    channels = block_width * lax.axis_size("tp")
    hidden = tokens
    full_value, full_gate, full_out = (
        lax.all_gather(value_proj, "sp", axis=1, tiled=True),
        lax.all_gather(gate_proj, "sp", axis=1, tiled=True),
        lax.all_gather(out_proj, "sp", axis=2, tiled=True),
    )
    for layer_index in range(layer_count):
        wide_state = hidden.astype(jnp.float32)
        scale = lax.rsqrt(jnp.mean(wide_state * wide_state, axis=-1, keepdims=True) + epsilon)
        normed = (wide_state * scale * pre_gain[layer_index]).astype(jnp.bfloat16)
        value_acc = jnp.dot(normed, full_value[layer_index], preferred_element_type=jnp.float32)
        gate_acc = jnp.dot(normed, full_gate[layer_index], preferred_element_type=jnp.float32)
        value_half = value_acc.astype(jnp.bfloat16)
        gate_half = gate_acc.astype(jnp.bfloat16)
        gated_rows = (
            value_half.astype(jnp.float32) * jax.nn.sigmoid(gate_half.astype(jnp.float32))
        ).astype(jnp.bfloat16)
        prev_rows, prev_docs = passed_along(
            (gated_rows[row_count - reach_rows :], doc_ids[row_count - reach_rows :]), "sp", 1
        )
        padded = jnp.concatenate([prev_rows, gated_rows]).astype(jnp.float32)
        padded_docs = jnp.concatenate([prev_docs, doc_ids])
        conv_out = jnp.zeros((row_count, block_width), jnp.float32)
        for offset in range(tap_count):
            first_row = reach_rows - offset
            same_doc = (padded_docs[first_row : first_row + row_count] == doc_ids)[:, None]
            term = (
                conv_taps[layer_index, offset][None, :] * padded[first_row : first_row + row_count]
            )
            conv_out = conv_out + jnp.where(same_doc, term, jnp.float32(0.0))
        row_sums, square_sums = lax.psum(
            (jnp.sum(conv_out, axis=1), jnp.sum(conv_out * conv_out, axis=1)), "tp"
        )
        row_mean = (row_sums / channels)[:, None]
        row_var = (square_sums / channels)[:, None] - row_mean * row_mean
        normalized = (
            norm_gain[layer_index] * (conv_out - row_mean) * lax.rsqrt(row_var + epsilon)
            + norm_shift[layer_index]
        )
        activated = jax.nn.silu(normalized).astype(jnp.bfloat16)
        partial_value = jnp.dot(
            activated, full_out[layer_index], preferred_element_type=jnp.float32
        )
        summed = lax.psum(partial_value.astype(jnp.bfloat16), "tp")
        hidden = (hidden.astype(jnp.float32) + summed.astype(jnp.float32)).astype(jnp.bfloat16)
    return hidden


def suits_kernel(n, m, tokens, value_proj, out_proj, conv_taps):
    rows, width = tokens.shape
    depth, block = value_proj.shape[1:]
    return (
        n % 2 == 0 and 4 <= n <= 16 and HALO <= GATE_ROWS and m % 2 == 0 and m >= 4 and rows % 128 == 0 and width % 256 == 0
        and depth % 32 == 0 and block == 256 and out_proj.shape[2] % 256 == 0
        and conv_taps.shape[1] - 1 <= HALO
    )


def solution(mesh):
    n, m = mesh.shape["sp"], mesh.shape["tp"]

    def body(tokens, doc_ids, pre_gain, value_proj, gate_proj, out_proj, conv_taps, norm_gain, norm_shift):
        chosen = on_device
        if suits_kernel(n, m, tokens, value_proj, out_proj, conv_taps):
            chosen = functools.partial(fused_on_device, n, m)
        return chosen(tokens, doc_ids, pre_gain, value_proj, gate_proj, out_proj, conv_taps, norm_gain, norm_shift)

    return jax.shard_map(
        body,
        mesh=mesh,
        in_specs=(
            P("sp", None),
            P("sp"),
            P(),
            P(None, "sp", "tp"),
            P(None, "sp", "tp"),
            P(None, "tp", "sp"),
            P(None, None, "tp"),
            P(None, "tp"),
            P(None, "tp"),
        ),
        out_specs=P("sp", None),
        check_vma=False,
    )
```

```python
import functools
import jax
import jax.numpy as jnp
from jax import lax
from jax.experimental import pallas as pl
from jax.experimental.pallas import tpu as pltpu
from jax.sharding import PartitionSpec as P

epsilon = 1e-06
MESH = pl.DeviceIdType.MESH
HALO = 32
CONV_ROWS = 64
GATE_ROWS = 64
MARKS = [2, 1, 1, 1, 1, 1, 1]


def fused_kernel(
    n, m, reach, layers,
    tok_hbm, doc_hbm, gain_hbm, v_hbm, g_hbm, o_hbm, tap_hbm, ng_hbm, ns_hbm,
    out_ref, tok_ref, doc_ref, gain_ref, v_ref, g_ref, o_ref, tap_ref, ng_ref, ns_ref,
    w, oall, normed, acc, padded, pdoc, run, ghalo, halo_in, doc_in, doc_tail,
    stat, stats, scales, conv, act, psend, precv, hid,
    rsend, rrecv, osend, orecv, hsend, hrecv, ssend, srecv, csend, crecv, xsend, xrecv, gsend, grecv, lsem,
):
    me = lax.axis_index("sp")
    t = lax.axis_index("tp")
    q, c = t // 2, t % 2
    pairs = m // 2
    half_n = n // 2
    rows, width = tok_ref.shape
    depth, block = v_ref.shape[1], v_ref.shape[2]
    owidth = o_ref.shape[2]
    hb, ho = block // 2, owidth // 2
    channels = block * m

    def index_of(position):
        position = (position + 2 * n) % n
        return jnp.where(position < half_n, 2 * position, 2 * (n - 1 - position) + 1)

    my_pos = jnp.where(me % 2 == 0, me // 2, n - 1 - me // 2)
    right, left = index_of(my_pos + 1), index_of(my_pos - 1)
    following = (me + 1) % n

    barrier = pltpu.get_barrier_semaphore()
    for other in (right, left):
        pl.semaphore_signal(barrier, inc=1, device_id={"sp": other}, device_id_type=MESH)
    for k in range(1, m):
        pl.semaphore_signal(barrier, inc=1, device_id={"tp": (t + k) % m}, device_id_type=MESH)
    loads = [pltpu.make_async_copy(src, dst, lsem.at[index]) for index, (src, dst) in enumerate(
        ((v_hbm, v_ref), (g_hbm, g_ref), (o_hbm, o_ref), (ng_hbm, ng_ref), (ns_hbm, ns_ref),
         (tok_hbm, tok_ref), (gain_hbm, gain_ref), (doc_hbm, doc_ref), (tap_hbm, tap_ref)))]
    for load in loads:
        load.start()
    pl.semaphore_wait(barrier, 1 + m)

    def to_sp(src, dst, send, recv, target):
        return pltpu.make_async_remote_copy(
            src_ref=src, dst_ref=dst, send_sem=send, recv_sem=recv,
            device_id={"sp": target}, device_id_type=MESH)

    def to_tp(src, dst, send, recv, target):
        return pltpu.make_async_remote_copy(
            src_ref=src, dst_ref=dst, send_sem=send, recv_sem=recv,
            device_id={"tp": target}, device_id_type=MESH)

    def owner_at(way, distance):
        return index_of(my_pos - distance if way == 0 else my_pos + distance)

    def held(layer, kind, owner, first=0, count=2):
        if kind < 2:
            return w.at[layer, kind, pl.ds(pl.multiple_of(owner * depth, depth), depth), pl.ds(first * hb, count * hb)]
        return oall.at[layer, pl.ds(pl.multiple_of(q * block, block), block),
                       pl.ds(pl.multiple_of(owner * owidth + first * ho, ho), count * ho)]

    def several(layer, kind, count):
        if kind < 2:
            return w.at[layer, kind, pl.ds(0, count * depth)]
        return oall.at[layer, pl.ds(pl.multiple_of(q * block, block), block), pl.ds(0, count * owidth)]

    def ring_copy(layer, kind, way, slot, src, dst):
        return to_sp(src, dst, rsend.at[layer, kind], rrecv.at[layer, kind, slot], right if way == 0 else left)

    def spread_copy(layer, k, src, dst):
        return to_tp(src, dst, osend.at[layer, k], orecv.at[layer, q], 2 * ((q + k) % pairs) + c)

    def advance_one(layer, kind, step):
        def land(slot, count):
            landed = several(layer, kind, count)
            ring_copy(layer, kind, 0, slot, landed, landed).wait_recv()

        def send(way, slot, first, count):
            owner = owner_at(way, step)
            dst = held(layer, kind, owner, first, count)
            if step > 0:
                ring_copy(layer, kind, way, slot, dst, dst).start()
            elif kind == 2:
                ring_copy(layer, kind, way, slot, o_ref.at[layer, :, pl.ds(first * ho, count * ho)], dst).start()
            else:
                for piece in range(first, first + count):
                    ring_copy(layer, kind, way, slot, (v_ref, g_ref)[piece].at[layer, :, pl.ds(kind * hb, hb)],
                              held(layer, kind, owner, piece, 1)).start()

        if step > 0:
            land(step - 1, 2 if step < half_n - 1 else 1)
        for way in range(2):
            if step < half_n - 2:
                send(way, step, 0, 2)
            elif step < half_n:
                send(way, step, way, 1)
        if step == half_n - 2:
            for way in range(2):
                send(way, half_n, 1 - way, 1)
        if step == half_n - 1:
            land(half_n, 1)
        if kind == 2 and step > 0:
            for way in range(2 if step < half_n else 1):
                for k in range(1, pairs):
                    part = held(layer, 2, owner_at(way, step))
                    spread_copy(layer, k, part, part).start()

    entries = []
    for layer in range(layers):
        for step in range(half_n + 1):
            for kind, (first, base, pace) in enumerate(
                    ((12.2, 11.7, 3.2), (13.3, 12.7, 3.2), (10.5, 10.55, 2.65)) if layer
                    else ((0, 0, 3), (1, 1, 3), (0.5, 0.5, 3))):
                shift = 11.5 * max(layer - 1, 0)
                entries.append((shift + (base + pace * step if step else first), layer, kind, step))
    pending = [entry[1:] for entry in sorted(entries)]

    def tend(count):
        for _ in range(count):
            if pending:
                advance_one(*pending.pop(0))

    def advance(*target):
        while target in pending:
            advance_one(*pending.pop(0))

    def drain(layer):
        for kind in range(3):
            ref = several(layer, kind, n - 1)
            ring_copy(layer, kind, 0, 0, ref, ref).wait_send()
        for k in range(1, pairs):
            ref = several(layer, 2, n)
            spread_copy(layer, k, ref, ref).wait_send()

    def keep_own(layer):
        row = pl.ds(pl.multiple_of(me * depth, depth), depth)
        for kind in range(2):
            w[layer, kind, row, pl.ds(0, hb)] = v_ref[layer, :, kind * hb:(kind + 1) * hb]
            w[layer, kind, row, pl.ds(hb, hb)] = g_ref[layer, :, kind * hb:(kind + 1) * hb]
        oall[layer, pl.ds(pl.multiple_of(q * block, block), block),
             pl.ds(pl.multiple_of(me * owidth, owidth), owidth)] = o_ref[layer]

    for load in loads[:5]:
        load.wait()
    tend(3)
    for layer in range(layers):
        for k in range(1, pairs):
            spread_copy(layer, k, o_ref.at[layer], held(layer, 2, me)).start()
    gain_copies = []
    for k in range(1, pairs):
        for index, src in enumerate((ng_ref, ns_ref)):
            to_tp(src, scales.at[q, index], gsend.at[k], grecv.at[q], 2 * ((q + k) % pairs) + c).start()
        gain_copies.append(to_tp(scales.at[q], scales.at[q], gsend.at[k], grecv.at[q], 2 * ((q + k) % pairs) + c))
    scales[q, 0] = ng_ref[...]
    scales[q, 1] = ns_ref[...]

    for load in loads[5:]:
        load.wait()

    def doc_block(i):
        row = doc_ref[pl.ds(i, 1), :].astype(jnp.float32)
        return jnp.transpose(jnp.broadcast_to(row, (128, 128)))

    doc_tail[...] = doc_block(rows // 128 - 1)[128 - HALO:]
    doc_copy = to_sp(doc_tail, doc_in, hsend.at[2 * layers], hrecv.at[2 * layers], following)

    for i in range(rows // 128):
        pdoc[pl.ds(HALO + i * 128, 128), :] = doc_block(i)
    pdoc[pl.ds(0, HALO), :] = jnp.full((HALO, 128), -1.0, jnp.float32)

    def norm_rows(layer, source):
        @pl.loop(0, rows // 32)
        def _(i):
            span = pl.ds(pl.multiple_of(i * 32, 32), 32)
            wide = source[span, :].astype(jnp.float32)
            scale = lax.rsqrt(jnp.mean(wide * wide, axis=-1, keepdims=True) + epsilon)
            normed[span, :] = (wide * scale * gain_ref[pl.ds(layer, 1), :]).astype(jnp.bfloat16)

    norm_rows(0, tok_ref)
    for layer in range(layers):
        keep_own(layer)

    @pl.when(me == 0)
    def _():
        halo_in[...] = jnp.zeros(halo_in.shape, halo_in.dtype)


    def count_runs():
        for k in range(1, pairs):
            peer = (q + k) % pairs
            to_tp(scales.at[peer], scales.at[peer], gsend.at[k], grecv.at[peer], 2 * peer + c).wait_recv()

        @pl.when(me > 0)
        def _():
            doc_copy.wait_recv()
            pdoc[pl.ds(0, HALO), :] = doc_in[...]

        @pl.loop(0, rows // CONV_ROWS)
        def _(i):
            base = pl.multiple_of(i * CONV_ROWS, CONV_ROWS)
            mine = pdoc[pl.ds(base + HALO, CONV_ROWS), :]
            count = jnp.zeros((CONV_ROWS, 128), jnp.int32)
            for j in range(1, reach + 1):
                count = count + (pdoc[pl.ds(base + (HALO - j), CONV_ROWS), :] == mine).astype(jnp.int32)
            run[pl.ds(base, CONV_ROWS), :] = count

    lane = lax.broadcasted_iota(jnp.int32, (CONV_ROWS, 128), 1)
    chunks = rows // 128
    order = list(range(1, chunks)) + [0]
    partner = 2 * q + 1 - c

    def layer_step(layer, source, target):
        last = layer + 1 == layers
        marks = MARKS[:]

        def pause():
            if not last and marks:
                tend(marks.pop(0))

        def halo_copy(kind):
            return to_sp(ghalo.at[layer, kind], halo_in.at[layer, kind],
                         hsend.at[2 * layer + kind], hrecv.at[2 * layer + kind], following)

        def gate_half(kind):
            if layer == 0:
                acc[kind] = jnp.dot(normed[...], w[layer, kind], preferred_element_type=jnp.float32)

            def gate_rows(start):
                span = pl.ds(start, GATE_ROWS)
                value = acc[kind, span, pl.ds(0, hb)].astype(jnp.bfloat16).astype(jnp.float32)
                gate = acc[kind, span, pl.ds(hb, hb)].astype(jnp.bfloat16).astype(jnp.float32)
                gated = (value * jax.nn.sigmoid(gate)).astype(jnp.bfloat16)
                padded[kind, pl.ds(start + HALO, GATE_ROWS), :] = gated.astype(jnp.float32)
                return gated

            ghalo[layer, kind] = gate_rows(rows - GATE_ROWS)[GATE_ROWS - HALO:]
            pl.when(me < n - 1)(lambda: halo_copy(kind).start())

            for i in range(rows // GATE_ROWS - 1):
                gate_rows(i * GATE_ROWS)

        def take_halo(kind):
            pl.when(me > 0)(lambda: halo_copy(kind).wait_recv())
            padded[kind, pl.ds(0, HALO), :] = halo_in[layer, kind].astype(jnp.float32)

        def conv_rows(kind, first, end):
            cols = pl.ds(kind * hb, hb)

            for i in range(first, end):
                base = i * CONV_ROWS
                span = pl.ds(base, CONV_ROWS)
                count = run[span, :]
                total = tap_ref[0, pl.ds(layer, 1), cols] * padded[kind, pl.ds(base + HALO, CONV_ROWS), :]
                for j in range(1, reach + 1):
                    term = tap_ref[j, pl.ds(layer, 1), cols] * padded[kind, pl.ds(base + (HALO - j), CONV_ROWS), :]
                    total = total + jnp.where(count >= j, term, jnp.float32(0.0))
                conv[layer, q, span, cols] = total.astype(jnp.bfloat16)
                sums = jnp.where(
                    lane == 0, jnp.sum(total, axis=1, keepdims=True),
                    jnp.where(lane == 1, jnp.sum(total * total, axis=1, keepdims=True), jnp.float32(0.0)))
                if kind:
                    sums = sums + stat[span, :]
                stat[span, :] = sums

        def conv_copies(kind, chunk):
            part = conv.at[layer, q, pl.ds(chunk * 128, 128), pl.ds(kind * hb, hb)]
            for k in range(1, pairs):
                to_tp(part, part, csend.at[layer], crecv.at[layer, chunk], 2 * ((q + k) % pairs) + c).start()

        def conv_landed(chunk):
            part = conv.at[layer, pl.ds(0, pairs - 1), pl.ds(chunk * 128, 128)]
            return to_tp(part, part, csend.at[layer], crecv.at[layer, chunk], partner)

        def stat_copies(chunk):
            part = stats.at[layer, chunk, t]
            for k in range(1, m):
                to_tp(part, part, ssend.at[layer], srecv.at[layer, chunk], (t + k) % m).start()

        def stats_landed(chunk):
            part = stats.at[layer, chunk, pl.ds(0, m - 1)]
            return to_tp(part, part, ssend.at[layer], srecv.at[layer, chunk], partner)

        def swap_copy(chunk):
            span = pl.ds(chunk * 128, 128)
            return to_tp(psend.at[layer, span], precv.at[layer, span], xsend.at[layer],
                         xrecv.at[layer, chunk], partner)

        def first_rows(chunk):
            conv_rows(0, 2 * chunk, 2 * chunk + 2)
            if not last or chunk == order[0]:
                conv_copies(0, chunk)

        def absorb(kind, step):
            for way in range(2 if 0 < step < half_n else 1):
                owner = owner_at(way, step)
                span = pl.ds(pl.multiple_of(owner * depth, depth), depth)
                part = jnp.dot(normed[:, span], w[layer, kind, span, :], preferred_element_type=jnp.float32)
                acc[kind] = acc[kind] + part if step else part

        def gather(kind):
            while (layer, kind, half_n) in pending:
                entry = pending.pop(0)
                advance_one(*entry)
                if layer and entry[0] == layer and entry[1] < 2:
                    absorb(*entry[1:])

        if layer:
            for step in range(half_n + 1):
                for kind in range(2):
                    if (layer, kind, step) not in pending:
                        absorb(kind, step)
        gather(0)
        if layer == 0:
            pl.when(me < n - 1)(doc_copy.start)
        gate_half(0)
        if layer == 0:
            advance(layer, 2, half_n)
            pause()
            count_runs()
        if last:
            for chunk in order[:-1]:
                first_rows(chunk)
        gather(1)
        gate_half(1)
        if not last:
            pause()
            for chunk in order[:-1]:
                first_rows(chunk)
        for chunk in order:
            if chunk == 0:
                conv_rows(0, 1, 2)
                conv_rows(1, 1, 2)
                take_halo(0)
                conv_rows(0, 0, 1)
                conv_copies(0, 0)
                pause()
                take_halo(1)
                conv_rows(1, 0, 1)
            else:
                conv_rows(1, 2 * chunk, 2 * chunk + 2)
            stats[layer, chunk, t] = jnp.transpose(stat[pl.ds(chunk * 128, 128), :])[:8]
            stat_copies(chunk)
            if last and chunk in order[1:-1]:
                conv_copies(0, chunk)
            conv_copies(1, chunk)

        pause()
        gains = [scales[p, 0, pl.ds(layer, 1), :] for p in range(pairs)]
        shifts = [scales[p, 1, pl.ds(layer, 1), :] for p in range(pairs)]
        for chunk in order:
            stats_landed(chunk).wait_recv()
            summed = stats[layer, chunk, 0]
            for who in range(1, m):
                summed = summed + stats[layer, chunk, who]
            both = jnp.transpose(jnp.concatenate([summed, jnp.zeros((120, 128), jnp.float32)], axis=0))
            row_mean = both[:, 0:1] / channels
            row_var = both[:, 1:2] / channels - row_mean * row_mean
            row_scale = lax.rsqrt(row_var + epsilon)
            conv_landed(chunk).wait_recv()
            span = pl.ds(chunk * 128, 128)
            for p in range(pairs):
                normalized = gains[p] * (conv[layer, p, span, :].astype(jnp.float32) - row_mean) * row_scale + shifts[p]
                act[span, pl.ds(p * block, block)] = jax.nn.silu(normalized).astype(jnp.bfloat16)
            if chunk == order[0]:
                advance(layer, 2, half_n)
                for k in range(1, pairs):
                    peer = (q + k) % pairs
                    part = oall.at[layer, pl.ds(pl.multiple_of(peer * block, block), block)]
                    to_tp(part, part, osend.at[layer, k], orecv.at[layer, peer], t).wait_recv()
            psend[layer, span, :] = jnp.dot(
                act[span, :], oall[layer], preferred_element_type=jnp.float32).astype(jnp.bfloat16)
            swap_copy(chunk).start()
            if chunk == order[0]:
                pause()

        pause()
        if last:
            for each in range(layers):
                drain(each)
            for copy in gain_copies:
                copy.wait_send()
            pl.when(me < n - 1)(doc_copy.wait_send)
        for chunk in order:
            swap_copy(chunk).wait_recv()

            @pl.loop(0, 128 // 32, unroll=True)
            def _(i, chunk=chunk):
                span = pl.ds(pl.multiple_of(chunk * 128 + i * 32, 32), 32)
                branch = (psend[layer, span, :].astype(jnp.float32)
                          + precv[layer, span, :].astype(jnp.float32)).astype(jnp.bfloat16)
                total = (source[span, :].astype(jnp.float32) + branch.astype(jnp.float32)).astype(jnp.bfloat16)
                target[span, :] = total
                if not last:
                    wide = total.astype(jnp.float32)
                    scale = lax.rsqrt(jnp.mean(wide * wide, axis=-1, keepdims=True) + epsilon)
                    normed[span, :] = (wide * scale * gain_ref[pl.ds(layer + 1, 1), :]).astype(jnp.bfloat16)

        for refs, sem in ((stats.at[layer, :, pl.ds(0, m - 1)], ssend), (conv.at[layer, pl.ds(0, pairs - 1)], csend),
                          (psend.at[layer], xsend)):
            to_tp(refs, refs, sem.at[layer], xrecv.at[layer, 0], partner).wait_send()
        for kind in range(2):
            pl.when(me < n - 1)(lambda kind=kind: halo_copy(kind).wait_send())

    for layer in range(layers):
        layer_step(layer, tok_ref if layer == 0 else hid.at[layer - 1],
                   out_ref if layer + 1 == layers else hid.at[layer])


def fused_on_device(n, m, tokens, doc_ids, pre_gain, value_proj, gate_proj, out_proj, conv_taps, norm_gain, norm_shift):
    rows, width = tokens.shape
    layers, depth, block = value_proj.shape
    owidth = out_proj.shape[2]
    reach = conv_taps.shape[1] - 1
    pairs, chunks = m // 2, rows // 128
    docs = doc_ids.reshape(rows // 128, 128)
    bf16, f32, i32 = jnp.bfloat16, jnp.float32, jnp.int32
    dma = pltpu.SemaphoreType.DMA
    vmem = pl.BlockSpec(memory_space=pltpu.VMEM)
    hbm = pl.BlockSpec(memory_space=pltpu.HBM)
    return pl.pallas_call(
        functools.partial(fused_kernel, n, m, reach, layers),
        out_shape=pltpu.VMEM((rows, width), bf16),
        in_specs=[hbm] * 9,
        out_specs=vmem,
        scratch_shapes=[
            pltpu.VMEM((rows, width), bf16), pltpu.VMEM(docs.shape, i32), pltpu.VMEM(pre_gain.shape, f32),
            pltpu.VMEM(value_proj.shape, bf16), pltpu.VMEM(gate_proj.shape, bf16), pltpu.VMEM(out_proj.shape, bf16),
            pltpu.VMEM((reach + 1, layers, block), f32), pltpu.VMEM(norm_gain.shape, f32), pltpu.VMEM(norm_shift.shape, f32),
            pltpu.VMEM((layers, 2, n * depth, block), bf16),
            pltpu.VMEM((layers, pairs * block, n * owidth), bf16),
            pltpu.VMEM((rows, width), bf16),
            pltpu.VMEM((2, rows, block), f32),
            pltpu.VMEM((2, rows + HALO, block // 2), f32),
            pltpu.VMEM((rows + HALO, 128), f32),
            pltpu.VMEM((rows, 128), i32),
            pltpu.VMEM((layers, 2, HALO, block // 2), bf16),
            pltpu.VMEM((layers, 2, HALO, block // 2), bf16),
            pltpu.VMEM((HALO, 128), f32),
            pltpu.VMEM((HALO, 128), f32),
            pltpu.VMEM((rows, 128), f32),
            pltpu.VMEM((layers, chunks, m, 8, 128), f32),
            pltpu.VMEM((pairs, 2, layers, block), f32),
            pltpu.VMEM((layers, pairs, rows, block), bf16),
            pltpu.VMEM((rows, pairs * block), bf16),
            pltpu.VMEM((layers, rows, width), bf16),
            pltpu.VMEM((layers, rows, width), bf16),
            pltpu.VMEM((max(1, layers - 1), rows, width), bf16),
            dma((layers, 3)), dma((layers, 3, n // 2 + 1)),
            dma((layers, pairs)), dma((layers, pairs)),
            dma((2 * layers + 1,)), dma((2 * layers + 1,)),
            dma((layers,)), dma((layers, chunks)),
            dma((layers,)), dma((layers, chunks)),
            dma((layers,)), dma((layers, chunks)),
            dma((pairs,)), dma((pairs,)), dma((9,)),
        ],
        compiler_params=pltpu.CompilerParams(
            collective_id=0, has_side_effects=True, vmem_limit_bytes=60 * 1024 * 1024),
    )(tokens, docs, pre_gain, value_proj, gate_proj, out_proj, jnp.transpose(conv_taps, (1, 0, 2)), norm_gain, norm_shift)


def passed_along(value, axis, steps):
    count = lax.axis_size(axis)
    first, last = (max(0, -steps), min(count, count - steps))
    return lax.ppermute(value, axis, [(source, source + steps) for source in range(first, last)])


def on_device(
    tokens, doc_ids, pre_gain, value_proj, gate_proj, out_proj, conv_taps, norm_gain, norm_shift
):
    layer_count = value_proj.shape[0]
    tap_count = conv_taps.shape[1]
    reach_rows = tap_count - 1
    row_count = tokens.shape[0]
    block_width = conv_taps.shape[2]
    channels = block_width * lax.axis_size("tp")
    hidden = tokens
    full_value, full_gate, full_out = (
        lax.all_gather(value_proj, "sp", axis=1, tiled=True),
        lax.all_gather(gate_proj, "sp", axis=1, tiled=True),
        lax.all_gather(out_proj, "sp", axis=2, tiled=True),
    )
    for layer_index in range(layer_count):
        wide_state = hidden.astype(jnp.float32)
        scale = lax.rsqrt(jnp.mean(wide_state * wide_state, axis=-1, keepdims=True) + epsilon)
        normed = (wide_state * scale * pre_gain[layer_index]).astype(jnp.bfloat16)
        value_acc = jnp.dot(normed, full_value[layer_index], preferred_element_type=jnp.float32)
        gate_acc = jnp.dot(normed, full_gate[layer_index], preferred_element_type=jnp.float32)
        value_half = value_acc.astype(jnp.bfloat16)
        gate_half = gate_acc.astype(jnp.bfloat16)
        gated_rows = (
            value_half.astype(jnp.float32) * jax.nn.sigmoid(gate_half.astype(jnp.float32))
        ).astype(jnp.bfloat16)
        prev_rows, prev_docs = passed_along(
            (gated_rows[row_count - reach_rows :], doc_ids[row_count - reach_rows :]), "sp", 1
        )
        padded = jnp.concatenate([prev_rows, gated_rows]).astype(jnp.float32)
        padded_docs = jnp.concatenate([prev_docs, doc_ids])
        conv_out = jnp.zeros((row_count, block_width), jnp.float32)
        for offset in range(tap_count):
            first_row = reach_rows - offset
            same_doc = (padded_docs[first_row : first_row + row_count] == doc_ids)[:, None]
            term = (
                conv_taps[layer_index, offset][None, :] * padded[first_row : first_row + row_count]
            )
            conv_out = conv_out + jnp.where(same_doc, term, jnp.float32(0.0))
        row_sums, square_sums = lax.psum(
            (jnp.sum(conv_out, axis=1), jnp.sum(conv_out * conv_out, axis=1)), "tp"
        )
        row_mean = (row_sums / channels)[:, None]
        row_var = (square_sums / channels)[:, None] - row_mean * row_mean
        normalized = (
            norm_gain[layer_index] * (conv_out - row_mean) * lax.rsqrt(row_var + epsilon)
            + norm_shift[layer_index]
        )
        activated = jax.nn.silu(normalized).astype(jnp.bfloat16)
        partial_value = jnp.dot(
            activated, full_out[layer_index], preferred_element_type=jnp.float32
        )
        summed = lax.psum(partial_value.astype(jnp.bfloat16), "tp")
        hidden = (hidden.astype(jnp.float32) + summed.astype(jnp.float32)).astype(jnp.bfloat16)
    return hidden


def suits_kernel(n, m, tokens, value_proj, out_proj, conv_taps):
    rows, width = tokens.shape
    depth, block = value_proj.shape[1:]
    return (
        n % 2 == 0 and 4 <= n <= 16 and HALO <= GATE_ROWS and m % 2 == 0 and m >= 4 and rows % 128 == 0 and width % 256 == 0
        and depth % 32 == 0 and block == 256 and out_proj.shape[2] % 256 == 0
        and conv_taps.shape[1] - 1 <= HALO
    )


def solution(mesh):
    n, m = mesh.shape["sp"], mesh.shape["tp"]

    def body(tokens, doc_ids, pre_gain, value_proj, gate_proj, out_proj, conv_taps, norm_gain, norm_shift):
        chosen = on_device
        if suits_kernel(n, m, tokens, value_proj, out_proj, conv_taps):
            chosen = functools.partial(fused_on_device, n, m)
        return chosen(tokens, doc_ids, pre_gain, value_proj, gate_proj, out_proj, conv_taps, norm_gain, norm_shift)

    return jax.shard_map(
        body,
        mesh=mesh,
        in_specs=(
            P("sp", None),
            P("sp"),
            P(),
            P(None, "sp", "tp"),
            P(None, "sp", "tp"),
            P(None, "tp", "sp"),
            P(None, None, "tp"),
            P(None, "tp"),
            P(None, "tp"),
        ),
        out_specs=P("sp", None),
        check_vma=False,
    )
```
